256 devices in a mesh: grp: 2 (over z), ep: 64 (over y, x), tp: 2 (over core).
Axes of the slice: x: 8, y: 8, z: 2, core: 2. Of those that a mesh axis runs over, the one named last changes fastest.
The devices are a block of a 8x8x16 slice.
Arguments:
- tokens: bfloat16 [4096, 2048], P(('grp', 'ep')), parts along dimension 0, may hold values from -6 to 6
- in_gain: bfloat16 [2048], replicated, may hold values from 0.099609375 to 1.8984375
- route_expert: int32 [4096, 6], P(('grp', 'ep')), parts along dimension 0, may hold values from 0 to 63, all different within a row; in each aligned block of 32 rows (0 to 31, 32 to 63, ...) at most 4 rows name the same one
- route_weight: float32 [4096, 6], P(('grp', 'ep')), parts along dimension 0, may hold values from 0.05 to 1
- gate_weight: bfloat16 [64, 2048, 768], P('ep', None, 'tp'), may hold values from -0.125 to 0.125
- up_weight: bfloat16 [64, 2048, 768], P('ep', None, 'tp'), may hold values from -0.125 to 0.125
- down_weight: bfloat16 [64, 768, 2048], P('ep', 'tp'), may hold values from -1 to 1
- shared_gate: bfloat16 [2048, 768], P(None, 'tp'), may hold values from -0.125 to 0.125
- shared_up: bfloat16 [2048, 768], P(None, 'tp'), may hold values from -0.125 to 0.125
- shared_down: bfloat16 [768, 2048], P('tp'), may hold values from -1 to 1
- out_gain: bfloat16 [2048], P('tp'), may hold values from 0.099609375 to 1.8984375
Outputs:
- mixed: bfloat16 [4096, 2048], P(('grp', 'ep'), 'tp'), parts along dimension 0
The draws below stay inside these ranges and needn't reach their ends.
There are 2 independent parts, one for each index of `grp`. The reference program is written for one: setup_inputs(seed, part) draws one part's arguments, and reference() takes and returns one part's arrays. A program takes and returns all parts, laid end to end along the dimension named above; an argument that names none is the same for every part. Nothing has to cross between parts.
Inputs may be any that keep to these rules, and one draw needn't show every extreme that they name: `route_expert`: each row names 6 different experts. Among the rows of one device no expert is named more than 4 times, a bound that some block reaches.
All inputs are finite; a program needn't handle non-finite values.
Results may differ from the reference program's by a relative error of at most 0.0077.
Values may be sent and summed in bfloat16 or wider, within the bound.
No kernel may reach another device: no remote copies, remote signals or barrier semaphores. Data moves between devices by JAX's collectives and lax.ppermute only.
A program may use at most 64 MiB of HBM per device.

```python
import math
import jax
import jax.numpy as jnp
import numpy as np
from jax import lax

D = 2048
FE = 768
FS = 768
TOPK = 6
TOK_DEV = 32
EXPERTS = 64
CAP = 4
TOKENS = 2048
N_EP = 64
N_TP = 2


def down_matrix(key, fan_in, copies, columns):
    position = jnp.arange(columns, dtype=jnp.float32) / columns
    draws = jnp.clip(jax.random.normal(key, (copies, fan_in, columns), jnp.float32), -4.0, 4.0)
    factor = 0.5 * 3.0 ** position
    return draws * factor[None, None, :] * fan_in ** (-0.5)


def draw_down_weight(key, part):
    return down_matrix(jax.random.fold_in(key, 11), FE, EXPERTS, D).astype(jnp.bfloat16)


def draw_shared_down(key, part):
    return down_matrix(jax.random.fold_in(key, 23), FS, 1, D)[0].astype(jnp.bfloat16)


def block_scale(own_key, extent, cuts, low, top_value):
    loudness, own = 1.0, jax.random.fold_in(own_key, 6)
    for dim, shards_of in cuts:
        heights = jnp.exp(jax.random.uniform(jax.random.fold_in(own, dim), (shards_of,), jnp.float32, low / len(cuts), top_value / len(cuts)))
        loudness = loudness * jnp.repeat(heights, extent[dim] // shards_of).reshape([-1 if axis == dim else 1 for axis in range(len(extent))])
    return loudness


def shared_out(rng, own, number, rows, number_of, top, reach, skew):
    ranking = jax.random.permutation(rng, number_of)
    crowded, ordinary = portions_of(number_of, rows * top, reach, skew, True), portions_of(number_of, rows * top, reach, skew, False)
    places = jnp.arange(number_of)

    def named(lengths, offset_by):
        used = int((lengths > 0).sum())
        fixed = max(1, used // 4)
        moved = fixed + (places - fixed + offset_by * (used - fixed)) % max(1, number_of - fixed)
        return jnp.zeros((number_of,), jnp.int32).at[ranking[jnp.where(places < fixed, places, moved)]].set(jnp.asarray(lengths, jnp.int32))

    lengths = jnp.where(number % 4 == 0, named(crowded, number // 4), named(ordinary, number - number // 4 - 1))
    mixed = jax.random.permutation(jax.random.fold_in(own, 3), number_of)
    giver, receiver = mixed[0:number_of // 2 * 2:2], mixed[1:number_of // 2 * 2:2]
    slack = jnp.minimum(lengths[giver] - 1, reach - lengths[receiver]) // 2
    slack = jnp.where((giver == ranking[0]) | (receiver == ranking[0]) | (lengths[receiver] == 0), 0, jnp.maximum(slack, 0))
    moved = jax.random.randint(jax.random.fold_in(own, 4), (number_of // 2,), 0, 1 << 20) % (slack + 1)
    lengths = lengths.at[giver].add(-moved).at[receiver].add(moved)
    members = jnp.searchsorted(jnp.cumsum(lengths), jnp.arange(rows * top), side="right").astype(jnp.int32)
    grid = members.reshape(top, rows).T
    grid = grid[jax.random.permutation(jax.random.fold_in(own, 1), rows)]
    offset_by = jax.random.randint(jax.random.fold_in(own, 2), (rows, 1), 0, top)
    return jnp.take_along_axis(grid, (jnp.arange(top)[None, :] + offset_by) % top, axis=1)


def portions_of(amount, total, reach, lean, full):
    weights = [(1 << 20) // math.isqrt(grade ** lean) + 1 for grade in range(1, amount + 1)]
    largest = reach if full else min(reach, max(-(-total // amount), total * weights[0] // sum(weights)))
    least = 1 if total - largest >= amount - 1 else 0
    holding, rest = [largest] + [least] * (amount - 1), total - largest - least * (amount - 1)
    while rest > 0:
        free = [i for i in range(1, amount) if holding[i] < largest] or [i for i in range(1, amount) if holding[i] < reach]
        pool, left = sum([weights[i] for i in free]), rest
        for i in free:
            extra = min(reach - holding[i], max(1, left * weights[i] // pool), rest)
            holding[i] = holding[i] + extra
            rest = rest - extra
    return np.array(holding)


def scatter_about(key, shape, spread, reach, shards=(), kind=jnp.bfloat16):
    loudness = block_scale(key, shape, shards, -0.22, 0.18) if shards else 1.0
    array = jax.random.normal(key, shape, jnp.float32) * spread * loudness
    return jnp.minimum(jnp.maximum(array, -reach), reach).astype(kind)


def setup_inputs(seed: int = 0, part: int = 0) -> dict:
    keys = jax.random.split(jax.random.key(seed), 12)
    own_keys = jax.random.split(jax.random.fold_in(keys[11], part), 12)
    tokens = scatter_about(own_keys[0], (TOKENS, D), 1.0, 6.0, ((0, 64),))
    in_gain = jnp.clip(1.0 + 0.18 * jax.random.normal(keys[1], (D,), jnp.float32), 0.099609375, 1.8984375).astype(jnp.bfloat16)
    route_expert_keys = jax.random.split(jax.random.fold_in(own_keys[2], 1), TOKENS // TOK_DEV)
    route_expert_turns = jax.random.permutation(jax.random.fold_in(own_keys[2], 3), TOKENS // TOK_DEV)
    route_expert = jax.vmap(lambda own, number: shared_out(jax.random.fold_in(own_keys[2], 2), own, number, TOK_DEV, EXPERTS, TOPK, CAP, 2))(route_expert_keys, route_expert_turns).reshape((TOKENS, TOPK))
    route_weight = jnp.clip(jnp.exp(math.log(1.0) - 2.9957323 * jax.random.uniform(own_keys[3], (TOKENS, TOPK), jnp.float32) ** block_scale(own_keys[3], (TOKENS, TOPK), ((0, 64),), -0.2, 0.2)), 0.05, 1.0)
    gate_weight = scatter_about(keys[4], (EXPERTS, D, FE), D ** -0.5, 0.125, ((0, 64), (2, 2)))
    up_weight = scatter_about(keys[5], (EXPERTS, D, FE), D ** -0.5, 0.125, ((0, 64), (2, 2)))
    down_weight = draw_down_weight(jax.random.fold_in(keys[11], 71), part)
    shared_gate = scatter_about(keys[7], (D, FS), D ** -0.5, 0.125, ((1, 2),))
    shared_up = scatter_about(keys[8], (D, FS), D ** -0.5, 0.125, ((1, 2),))
    shared_down = draw_shared_down(jax.random.fold_in(keys[11], 71), part)
    out_gain = jnp.clip(1.0 + 0.18 * jax.random.normal(keys[10], (D,), jnp.float32), 0.099609375, 1.8984375).astype(jnp.bfloat16)
    return dict(tokens=tokens, in_gain=in_gain, route_expert=route_expert, route_weight=route_weight, gate_weight=gate_weight, up_weight=up_weight, down_weight=down_weight, shared_gate=shared_gate, shared_up=shared_up, shared_down=shared_down, out_gain=out_gain)


EPSILON = 1e-06

def normalize(values, gain_vector):
    floats = values.astype(jnp.float32)
    scaled = floats * lax.rsqrt(lax.optimization_barrier(jnp.mean(floats * floats, axis=-1, keepdims=True)) + EPSILON)
    return (scaled * gain_vector.astype(jnp.float32)).astype(jnp.bfloat16)

def swiglu_hidden(inputs, gate_here, up_here):
    gate_value = jnp.dot(inputs, gate_here, preferred_element_type=jnp.float32)
    upward = jnp.dot(inputs, up_here, preferred_element_type=jnp.float32)
    return (jax.nn.silu(gate_value) * upward).astype(jnp.bfloat16)

def split_product(hidden, down_here, pieces):
    inner_width = hidden.shape[1] // pieces
    running = jnp.zeros((hidden.shape[0], down_here.shape[1]), jnp.float32)
    for portion in range(pieces):
        partial_value = jnp.dot(hidden[:, portion * inner_width:(portion + 1) * inner_width], down_here[portion * inner_width:(portion + 1) * inner_width], preferred_element_type=jnp.float32)
        running = running + lax.optimization_barrier(partial_value.astype(jnp.bfloat16)).astype(jnp.float32)
    return running.astype(jnp.bfloat16)

def slot_tables(routes_here, experts, capacity):
    picked_count = routes_here.shape[0] * routes_here.shape[1]
    flattened = routes_here.reshape(picked_count).astype(jnp.int32)
    onehot = (flattened[:, None] == jnp.arange(experts, dtype=jnp.int32)[None, :]).astype(jnp.int32)
    earlier = (jnp.cumsum(onehot, axis=0) - onehot).astype(jnp.int32)
    ranked = lax.optimization_barrier(jnp.sum(earlier * onehot, axis=1)).astype(jnp.int32)
    slot_index = flattened * capacity + ranked
    source_token = jnp.arange(picked_count, dtype=jnp.int32) // routes_here.shape[1]
    matches = slot_index[None, :] == jnp.arange(experts * capacity, dtype=jnp.int32)[:, None]
    filled = jnp.any(matches, axis=1)
    slot_owner = lax.optimization_barrier(jnp.sum(jnp.where(matches, source_token[None, :], 0), axis=1)).astype(jnp.int32)
    return (slot_index, filled, slot_owner)

def reference(tokens, in_gain, route_expert, route_weight, gate_weight, up_weight, down_weight, shared_gate, shared_up, shared_down, out_gain):
    capacity = CAP
    normed = normalize(tokens, in_gain)
    grouped = route_expert.reshape(N_EP, TOK_DEV, TOPK)
    slot_index, filled, slot_owner = jax.vmap(lambda routes_here: slot_tables(routes_here, EXPERTS, capacity))(grouped)
    per_device = normed.reshape(N_EP, TOK_DEV, D)
    outgoing = jax.vmap(lambda rows_here, chosen, filled_here: jnp.where(filled_here[:, None], rows_here[chosen], jnp.zeros((), jnp.bfloat16)))(per_device, slot_owner, filled)
    by_expert = outgoing.reshape(N_EP, EXPERTS, capacity, D).transpose(1, 0, 2, 3).reshape(EXPERTS, N_EP * capacity, D)

    def expert_pass(inputs):
        expert_rows, gate_here, up_here, down_here = inputs
        return split_product(swiglu_hidden(expert_rows, gate_here, up_here), down_here, N_TP)
    results = lax.map(expert_pass, (by_expert, gate_weight, up_weight, down_weight))
    returned = results.reshape(EXPERTS, N_EP, capacity, D).transpose(1, 0, 2, 3).reshape(N_EP, EXPERTS * capacity, D)
    picked = jax.vmap(lambda result_rows, chosen: result_rows[chosen])(returned, slot_index).astype(jnp.float32)
    picked = picked * route_weight.reshape(N_EP, TOK_DEV * TOPK)[:, :, None]
    routed = lax.optimization_barrier(jnp.sum(picked.reshape(TOKENS, TOPK, D), axis=1))
    shared = split_product(swiglu_hidden(normed, shared_gate, shared_up), shared_down, N_TP).astype(jnp.float32)
    combined = shared + routed
    scaled = combined * lax.rsqrt(lax.optimization_barrier(jnp.mean(combined * combined, axis=1, keepdims=True)) + EPSILON)
    return (scaled * out_gain.astype(jnp.float32)).astype(jnp.bfloat16)
```

```python
import functools

import jax
import jax.numpy as jnp
from jax import lax
from jax.experimental import pallas as pl
from jax.experimental.pallas import tpu as pltpu
from jax.sharding import PartitionSpec as P

EPSILON = 1e-06
F32 = jnp.float32
BF16 = jnp.bfloat16
VMEM = pltpu.VMEM


def whole():
    return pl.BlockSpec(memory_space=VMEM)


def iota(shape, dim):
    return lax.broadcasted_iota(jnp.int32, shape, dim)


def chosen(route, core, slots, pieces, experts, values=None):
    top, tokens = route.shape
    rows, lanes = experts * slots * pieces, pieces * tokens
    row, lane = iota((rows, lanes), 0), iota((rows, lanes), 1)
    expert = row // (slots * pieces)
    tiled = jnp.concatenate([route] * pieces, axis=1)
    hits = [tiled[k : k + 1] == expert for k in range(top)]
    named = functools.reduce(jnp.logical_or, hits)
    before, after = iota((lanes, lanes), 0), iota((lanes, lanes), 1)
    earlier = (before // tokens == after // tokens) & (before < after)
    ones = jnp.where(named, 1.0, 0.0).astype(BF16)
    rank = jnp.dot(ones, jnp.where(earlier, 1.0, 0.0).astype(BF16), preferred_element_type=F32)
    wanted = ((row // pieces) % slots + slots * core).astype(F32)
    keep = named & (rank == wanted) & (lane // tokens == row % pieces)
    if values is None:
        return jnp.where(keep, 1.0, 0.0)
    spread = jnp.concatenate([values] * pieces, axis=1)
    total = jnp.zeros((rows, lanes), F32)
    for k in range(top):
        total = jnp.where(hits[k], spread[k : k + 1], total)
    return jnp.where(keep, total, 0.0)


def dispatch_kernel(tokens_ref, gain_ref, route_ref, send_ref, normed_ref, *, slots, pieces, experts):
    core = lax.axis_index("tp")
    values = tokens_ref[...].astype(F32)
    scaled = values * lax.rsqrt(jnp.mean(values * values, axis=-1, keepdims=True) + EPSILON)
    normed = (scaled * gain_ref[...].astype(F32)).astype(BF16)
    normed_ref[...] = normed
    piece = normed.shape[1] // pieces
    stacked = jnp.concatenate([normed[:, q * piece : (q + 1) * piece] for q in range(pieces)], axis=0)
    pick = chosen(route_ref[...], core, slots, pieces, experts).astype(BF16)
    send_ref[...] = jnp.dot(pick, stacked, preferred_element_type=F32).astype(BF16)


def shared_kernel(
    normed_ref, gate_ref, up_ref, down_ref, route_ref, weight_ref, part_ref, mix_ref, *, slots, pieces, experts
):
    core = lax.axis_index("tp")
    normed = normed_ref[...]
    gate = jnp.dot(normed, gate_ref[...], preferred_element_type=F32)
    upward = jnp.dot(normed, up_ref[...], preferred_element_type=F32)
    hidden = (gate * jax.nn.sigmoid(gate) * upward).astype(BF16)
    tokens, piece = normed.shape[0], normed.shape[1] // pieces
    for q in range(pieces):
        part_ref[q * tokens : (q + 1) * tokens, :] = jnp.dot(
            hidden, down_ref[:, q * piece : (q + 1) * piece], preferred_element_type=F32
        )
    mix = chosen(route_ref[...], core, slots, pieces, experts, weight_ref[...]).T
    high = mix.astype(BF16)
    mix_ref[: mix.shape[0], :] = high
    mix_ref[mix.shape[0] :, :] = (mix - high.astype(F32)).astype(BF16)


def gathering(half, pieces):
    to, frm = iota((half * pieces, half * pieces), 0), iota((half * pieces, half * pieces), 1)
    return jnp.where(frm == (to % half) * pieces + to // half, 1.0, 0.0).astype(BF16)


def expert_kernel(
    rows_ref, gate_ref, up_ref, down_ref, gate2_ref, up2_ref, down2_ref, out_ref, *, pieces
):
    total = rows_ref.shape[0]
    rows, block = total // pieces, total // 2
    half = rows // 2
    piece = rows_ref.shape[1]
    order = gathering(half, pieces)
    parts = [
        jnp.dot(order, rows_ref[h * block : (h + 1) * block, :], preferred_element_type=F32).astype(BF16)
        for h in range(2)
    ]
    inputs = jnp.concatenate(
        [
            jnp.concatenate([parts[h][q * half : (q + 1) * half] for h in range(2)], axis=0)
            for q in range(pieces)
        ],
        axis=1,
    )
    hidden = []
    for g, u in ((gate_ref, up_ref), (gate2_ref, up2_ref)):
        gate = jnp.dot(inputs, g[...], preferred_element_type=F32)
        upward = jnp.dot(inputs, u[...], preferred_element_type=F32)
        hidden.append((gate * jax.nn.sigmoid(gate) * upward).astype(BF16))
    back = order.T
    results = []
    for q in range(pieces):
        span = slice(q * piece, (q + 1) * piece)
        results.append(
            (
                jnp.dot(hidden[0], down_ref[:, span], preferred_element_type=F32)
                + jnp.dot(hidden[1], down2_ref[:, span], preferred_element_type=F32)
            ).astype(BF16)
        )
    for h in range(2):
        lined = jnp.concatenate([r[h * half : (h + 1) * half] for r in results], axis=0)
        out_ref[h * block : (h + 1) * block, :] = jnp.dot(back, lined, preferred_element_type=F32).astype(BF16)


def combine_kernel(mix_ref, returned_ref, part_ref, out_ref):
    both = jnp.dot(mix_ref[...], returned_ref[...], preferred_element_type=F32)
    size = both.shape[0] // 2
    out_ref[...] = part_ref[...] + both[:size] + both[size:]


def closing_kernel(mine_ref, other_ref, gain_ref, out_ref, total_ref, *, pieces):
    core = lax.axis_index("tp")
    total = mine_ref[...] + other_ref[...]
    total_ref[...] = total
    tokens, piece = total.shape[0] // pieces, total.shape[1]
    squares = jnp.sum(total * total, axis=1, keepdims=True)
    squares = functools.reduce(jnp.add, [squares[q * tokens : (q + 1) * tokens] for q in range(pieces)])
    scale = lax.rsqrt(squares / (pieces * piece) + EPSILON)
    mine = out_ref.shape[1] // piece
    gain = gain_ref[...].astype(F32)
    for q in range(mine):
        start = pl.multiple_of((core * mine + q) * tokens, 8)
        values = total_ref[pl.ds(start, tokens), :] * scale
        out_ref[:, q * piece : (q + 1) * piece] = (values * gain[:, q * piece : (q + 1) * piece]).astype(BF16)


def body(
    tokens,
    in_gain,
    route_expert,
    route_weight,
    gate_weight,
    up_weight,
    down_weight,
    shared_gate,
    shared_up,
    shared_down,
    out_gain,
):
    experts, cores = lax.axis_size("ep"), lax.axis_size("tp")
    local_tokens, width = tokens.shape
    top_count = route_expert.shape[1]
    capacity = max(2, (local_tokens * top_count * 4 + 3 * experts - 1) // (3 * experts))
    slots = capacity // cores
    pieces = 8 // slots
    piece = width // pieces
    rows = experts * slots * pieces
    sizes = dict(slots=slots, pieces=pieces, experts=experts)
    params = pltpu.CompilerParams(vmem_limit_bytes=48 * 1024 * 1024)

    swap = [(i, (i + 1) % cores) for i in range(cores)]
    weights = (gate_weight[0], up_weight[0], down_weight[0])
    others = tuple(lax.ppermute(w, "tp", swap) for w in weights)

    send, normed = pl.pallas_call(
        functools.partial(dispatch_kernel, **sizes),
        out_shape=(
            jax.ShapeDtypeStruct((rows, piece), BF16),
            jax.ShapeDtypeStruct((local_tokens, width), BF16),
        ),
        in_specs=[whole()] * 3,
        out_specs=(whole(), whole()),
        name="dispatch",
    )(tokens, in_gain.reshape(1, width), route_expert.T)
    with jax.named_scope("outward"):
        arrived = lax.all_to_all(send.reshape(experts, slots * pieces, piece), "ep", 0, 0, tiled=True)

    part, mix = pl.pallas_call(
        functools.partial(shared_kernel, **sizes),
        out_shape=(
            jax.ShapeDtypeStruct((pieces * local_tokens, piece), F32),
            jax.ShapeDtypeStruct((2 * pieces * local_tokens, rows), BF16),
        ),
        in_specs=[whole()] * 6,
        out_specs=(whole(), whole()),
        compiler_params=params,
        name="shared",
    )(normed, shared_gate, shared_up, shared_down, route_expert.T, route_weight.T)

    results = pl.pallas_call(
        functools.partial(expert_kernel, pieces=pieces),
        out_shape=jax.ShapeDtypeStruct((rows, piece), BF16),
        in_specs=[whole()] * 7,
        out_specs=whole(),
        compiler_params=params,
        name="expert",
    )(arrived.reshape(rows, piece), *weights, *others)
    with jax.named_scope("homeward"):
        returned = lax.all_to_all(results.reshape(experts, slots * pieces, piece), "ep", 0, 0, tiled=True)

    mine = pl.pallas_call(
        combine_kernel,
        out_shape=jax.ShapeDtypeStruct((pieces * local_tokens, piece), F32),
        in_specs=[whole()] * 3,
        out_specs=whole(),
        name="combine",
    )(mix, returned.reshape(rows, piece), part)
    other = lax.ppermute(mine, "tp", swap)
    return pl.pallas_call(
        functools.partial(closing_kernel, pieces=pieces),
        out_shape=jax.ShapeDtypeStruct((local_tokens, out_gain.shape[0]), BF16),
        in_specs=[whole()] * 3,
        out_specs=whole(),
        scratch_shapes=[VMEM((pieces * local_tokens, piece), F32)],
        name="closing",
    )(mine, other, out_gain.reshape(1, -1))


def solution(mesh):
    return jax.shard_map(
        body,
        mesh=mesh,
        in_specs=(
            P(("grp", "ep"), None),
            P(),
            P(("grp", "ep"), None),
            P(("grp", "ep"), None),
            P("ep", None, "tp"),
            P("ep", None, "tp"),
            P("ep", "tp", None),
            P(None, "tp"),
            P(None, "tp"),
            P("tp", None),
            P("tp"),
        ),
        out_specs=P(("grp", "ep"), "tp"),
        check_vma=False,
    )
```

```python
import functools

import jax
import jax.numpy as jnp
from jax import lax
from jax.experimental import pallas as pl
from jax.experimental.pallas import tpu as pltpu
from jax.sharding import PartitionSpec as P

EPSILON = 1e-06
F32 = jnp.float32
BF16 = jnp.bfloat16
VMEM = pltpu.VMEM


def whole():
    return pl.BlockSpec(memory_space=VMEM)


def anywhere():
    return pl.BlockSpec(memory_space=pl.ANY)


def held(*arrays):
    return [pltpu.with_memory_space_constraint(a, VMEM) for a in arrays]


def far(*arrays):
    return [pltpu.with_memory_space_constraint(a, pltpu.HBM) for a in arrays]


def grant(mebibytes):
    return pltpu.CompilerParams(vmem_limit_bytes=mebibytes * 1024 * 1024)


def iota(shape, dim):
    return lax.broadcasted_iota(jnp.int32, shape, dim)


def chosen(route, core, slots, pieces, experts, values=None):
    top, tokens = route.shape
    rows, lanes = experts * slots * pieces, pieces * tokens
    row, lane = iota((rows, lanes), 0), iota((rows, lanes), 1)
    expert = row // (slots * pieces)
    tiled = jnp.concatenate([route] * pieces, axis=1)
    hits = [tiled[k : k + 1] == expert for k in range(top)]
    named = functools.reduce(jnp.logical_or, hits)
    before, after = iota((lanes, lanes), 0), iota((lanes, lanes), 1)
    earlier = (before // tokens == after // tokens) & (before < after)
    ones = jnp.where(named, 1.0, 0.0).astype(BF16)
    rank = jnp.dot(ones, jnp.where(earlier, 1.0, 0.0).astype(BF16), preferred_element_type=F32)
    wanted = ((row // pieces) % slots + slots * core).astype(F32)
    keep = named & (rank == wanted) & (lane // tokens == row % pieces)
    if values is None:
        return jnp.where(keep, 1.0, 0.0)
    spread = jnp.concatenate([values] * pieces, axis=1)
    total = jnp.zeros((rows, lanes), F32)
    for k in range(top):
        total = jnp.where(hits[k], spread[k : k + 1], total)
    return jnp.where(keep, total, 0.0)


def dispatch_kernel(
    tokens_hbm,
    gain_hbm,
    route_hbm,
    send_ref,
    normed_ref,
    tokens_ref,
    gain_ref,
    route_ref,
    sems,
    *,
    slots,
    pieces,
    experts,
):
    core = lax.axis_index("tp")
    loads = [
        pltpu.make_async_copy(src, dst, sems.at[i])
        for i, (src, dst) in enumerate(
            ((route_hbm, route_ref), (tokens_hbm, tokens_ref), (gain_hbm, gain_ref))
        )
    ]
    for load in loads:
        load.start()
    loads[0].wait()
    pick = chosen(route_ref[...], core, slots, pieces, experts).astype(BF16)
    loads[1].wait()
    loads[2].wait()
    values = tokens_ref[...].astype(F32)
    scaled = values * lax.rsqrt(jnp.mean(values * values, axis=-1, keepdims=True) + EPSILON)
    normed = (scaled * gain_ref[...].astype(F32)[None, :]).astype(BF16)
    normed_ref[...] = normed
    piece = normed.shape[1] // pieces
    stacked = jnp.concatenate([normed[:, q * piece : (q + 1) * piece] for q in range(pieces)], axis=0)
    send_ref[...] = jnp.dot(pick, stacked, preferred_element_type=F32).astype(BF16)


def shared_kernel(
    normed_ref, gate_ref, up_ref, down_ref, route_ref, weight_ref, part_ref, mix_ref, *, slots, pieces, experts
):
    core = lax.axis_index("tp")
    normed = normed_ref[...]
    gate = jnp.dot(normed, gate_ref[...], preferred_element_type=F32)
    upward = jnp.dot(normed, up_ref[...], preferred_element_type=F32)
    hidden = (gate * jax.nn.sigmoid(gate) * upward).astype(BF16)
    tokens, piece = normed.shape[0], normed.shape[1] // pieces
    for q in range(pieces):
        part_ref[q * tokens : (q + 1) * tokens, :] = jnp.dot(
            hidden, down_ref[:, q * piece : (q + 1) * piece], preferred_element_type=F32
        )
    mix = chosen(route_ref[...], core, slots, pieces, experts, weight_ref[...]).T
    high = mix.astype(BF16)
    mix_ref[: mix.shape[0], :] = high
    mix_ref[mix.shape[0] :, :] = (mix - high.astype(F32)).astype(BF16)


def gathering(half, pieces):
    to, frm = iota((half * pieces, half * pieces), 0), iota((half * pieces, half * pieces), 1)
    return jnp.where(frm == (to % half) * pieces + to // half, 1.0, 0.0).astype(BF16)


def expert_kernel(
    rows_ref,
    gate2_ref,
    up2_ref,
    down2_ref,
    gate_hbm,
    up_hbm,
    down_hbm,
    out_ref,
    gate_ref,
    up_ref,
    down_ref,
    sems,
    *,
    pieces,
):
    loads = [
        pltpu.make_async_copy(src, dst, sems.at[i])
        for i, (src, dst) in enumerate(((gate_hbm, gate_ref), (up_hbm, up_ref), (down_hbm, down_ref)))
    ]
    for load in loads:
        load.start()
    total = rows_ref.shape[0]
    rows, block = total // pieces, total // 2
    half = rows // 2
    piece = rows_ref.shape[1]
    order = gathering(half, pieces)
    parts = [
        jnp.dot(order, rows_ref[h * block : (h + 1) * block, :], preferred_element_type=F32).astype(BF16)
        for h in range(2)
    ]
    inputs = jnp.concatenate(
        [
            jnp.concatenate([parts[h][q * half : (q + 1) * half] for h in range(2)], axis=0)
            for q in range(pieces)
        ],
        axis=1,
    )
    hidden = []
    for own, (g, u) in enumerate(((gate2_ref, up2_ref), (gate_ref, up_ref))):
        if own:
            loads[0].wait()
            loads[1].wait()
        gate = jnp.dot(inputs, g[...], preferred_element_type=F32)
        upward = jnp.dot(inputs, u[...], preferred_element_type=F32)
        hidden.append((gate * jax.nn.sigmoid(gate) * upward).astype(BF16))
    back = order.T
    loads[2].wait()
    results = []
    for q in range(pieces):
        span = slice(q * piece, (q + 1) * piece)
        results.append(
            (
                jnp.dot(hidden[0], down2_ref[:, span], preferred_element_type=F32)
                + jnp.dot(hidden[1], down_ref[:, span], preferred_element_type=F32)
            ).astype(BF16)
        )
    for h in range(2):
        lined = jnp.concatenate([r[h * half : (h + 1) * half] for r in results], axis=0)
        out_ref[h * block : (h + 1) * block, :] = jnp.dot(back, lined, preferred_element_type=F32).astype(BF16)


def combine_kernel(mix_ref, returned_ref, part_ref, out_ref):
    both = jnp.dot(mix_ref[...], returned_ref[...], preferred_element_type=F32)
    size = both.shape[0] // 2
    out_ref[...] = part_ref[...] + both[:size] + both[size:]


def closing_kernel(mine_ref, other_ref, gain_ref, out_ref, total_ref, *, pieces):
    core = lax.axis_index("tp")
    total = mine_ref[...] + other_ref[...]
    total_ref[...] = total
    tokens, piece = total.shape[0] // pieces, total.shape[1]
    squares = jnp.sum(total * total, axis=1, keepdims=True)
    squares = functools.reduce(jnp.add, [squares[q * tokens : (q + 1) * tokens] for q in range(pieces)])
    scale = lax.rsqrt(squares / (pieces * piece) + EPSILON)
    mine = out_ref.shape[1] // piece
    gain = gain_ref[...].astype(F32)[None, :]
    for q in range(mine):
        start = pl.multiple_of((core * mine + q) * tokens, 8)
        values = total_ref[pl.ds(start, tokens), :] * scale
        out_ref[:, q * piece : (q + 1) * piece] = (values * gain[:, q * piece : (q + 1) * piece]).astype(BF16)


def body(
    tokens,
    in_gain,
    route_expert,
    route_weight,
    gate_weight,
    up_weight,
    down_weight,
    shared_gate,
    shared_up,
    shared_down,
    out_gain,
):
    experts, cores = lax.axis_size("ep"), lax.axis_size("tp")
    local_tokens, width = tokens.shape
    top_count = route_expert.shape[1]
    capacity = max(2, (local_tokens * top_count * 4 + 3 * experts - 1) // (3 * experts))
    slots = capacity // cores
    pieces = 8 // slots
    piece = width // pieces
    rows = experts * slots * pieces
    sizes = dict(slots=slots, pieces=pieces, experts=experts)

    swap = [(i, (i + 1) % cores) for i in range(cores)]
    weights = (gate_weight[0], up_weight[0], down_weight[0])
    others = tuple(lax.ppermute(w, "tp", swap) for w in weights)

    send, normed = pl.pallas_call(
        functools.partial(dispatch_kernel, **sizes),
        out_shape=(
            VMEM((rows, piece), BF16),
            VMEM((local_tokens, width), BF16),
        ),
        in_specs=[anywhere()] * 3,
        out_specs=(whole(), whole()),
        scratch_shapes=[
            VMEM(tokens.shape, BF16),
            VMEM(in_gain.shape, BF16),
            VMEM(route_expert.shape[::-1], jnp.int32),
            pltpu.SemaphoreType.DMA((3,)),
        ],
        compiler_params=grant(6),
        name="dispatch",
    )(*far(tokens, in_gain, route_expert.T))
    with jax.named_scope("outward"):
        arrived = lax.all_to_all(send.reshape(experts, slots * pieces, piece), "ep", 0, 0, tiled=True)

    part, mix = pl.pallas_call(
        functools.partial(shared_kernel, **sizes),
        out_shape=(
            VMEM((pieces * local_tokens, piece), F32),
            VMEM((2 * pieces * local_tokens, rows), BF16),
        ),
        in_specs=[whole()] * 6,
        out_specs=(whole(), whole()),
        compiler_params=grant(8),
        name="shared",
    )(*held(normed, shared_gate, shared_up, shared_down, route_expert.T, route_weight.T))

    results = pl.pallas_call(
        functools.partial(expert_kernel, pieces=pieces),
        out_shape=VMEM((rows, piece), BF16),
        in_specs=[whole()] * 4 + [anywhere()] * 3,
        out_specs=whole(),
        scratch_shapes=[VMEM(w.shape, BF16) for w in weights] + [pltpu.SemaphoreType.DMA((3,))],
        compiler_params=grant(12),
        name="expert",
    )(*held(arrived.reshape(rows, piece), *others), *far(*weights))
    with jax.named_scope("homeward"):
        returned = lax.all_to_all(results.reshape(experts, slots * pieces, piece), "ep", 0, 0, tiled=True)

    mine = pl.pallas_call(
        combine_kernel,
        out_shape=VMEM((pieces * local_tokens, piece), F32),
        in_specs=[whole()] * 3,
        out_specs=whole(),
        compiler_params=grant(4),
        name="combine",
    )(*held(mix, returned.reshape(rows, piece), part))
    other = lax.ppermute(mine, "tp", swap)
    return pl.pallas_call(
        functools.partial(closing_kernel, pieces=pieces),
        out_shape=jax.ShapeDtypeStruct((local_tokens, out_gain.shape[0]), BF16),
        in_specs=[whole()] * 3,
        out_specs=whole(),
        scratch_shapes=[VMEM((pieces * local_tokens, piece), F32)],
        compiler_params=grant(4),
        name="closing",
    )(*held(mine, other, out_gain))


def solution(mesh):
    return jax.shard_map(
        body,
        mesh=mesh,
        in_specs=(
            P(("grp", "ep"), None),
            P(),
            P(("grp", "ep"), None),
            P(("grp", "ep"), None),
            P("ep", None, "tp"),
            P("ep", None, "tp"),
            P("ep", "tp", None),
            P(None, "tp"),
            P(None, "tp"),
            P("tp", None),
            P("tp"),
        ),
        out_specs=P(("grp", "ep"), "tp"),
        check_vma=False,
    )
```

```python
import functools

import jax
import jax.numpy as jnp
from jax import lax
from jax.experimental import pallas as pl
from jax.experimental.pallas import tpu as pltpu
from jax.sharding import PartitionSpec as P

EPSILON = 1e-06
F32 = jnp.float32
BF16 = jnp.bfloat16
VMEM = pltpu.VMEM


def whole():
    return pl.BlockSpec(memory_space=VMEM)


def anywhere():
    return pl.BlockSpec(memory_space=pl.ANY)


def held(*arrays):
    return [pltpu.with_memory_space_constraint(a, VMEM) for a in arrays]


def far(*arrays):
    return [pltpu.with_memory_space_constraint(a, pltpu.HBM) for a in arrays]


def grant(mebibytes):
    return pltpu.CompilerParams(vmem_limit_bytes=mebibytes * 1024 * 1024)


def iota(shape, dim):
    return lax.broadcasted_iota(jnp.int32, shape, dim)


def chosen(route, core, slots, pieces, experts, values=None):
    top, tokens = route.shape
    rows, lanes = experts * slots * pieces, pieces * tokens
    row, lane = iota((rows, lanes), 0), iota((rows, lanes), 1)
    expert = row // (slots * pieces)
    tiled = jnp.concatenate([route] * pieces, axis=1)
    hits = [tiled[k : k + 1] == expert for k in range(top)]
    named = functools.reduce(jnp.logical_or, hits)
    before, after = iota((lanes, lanes), 0), iota((lanes, lanes), 1)
    earlier = (before // tokens == after // tokens) & (before < after)
    ones = jnp.where(named, 1.0, 0.0).astype(BF16)
    rank = jnp.dot(ones, jnp.where(earlier, 1.0, 0.0).astype(BF16), preferred_element_type=F32)
    wanted = ((row // pieces) % slots + slots * core).astype(F32)
    keep = named & (rank == wanted) & (lane // tokens == row % pieces)
    if values is None:
        return jnp.where(keep, 1.0, 0.0)
    spread = jnp.concatenate([values] * pieces, axis=1)
    total = jnp.zeros((rows, lanes), F32)
    for k in range(top):
        total = jnp.where(hits[k], spread[k : k + 1], total)
    return jnp.where(keep, total, 0.0)


def dispatch_kernel(
    tokens_hbm,
    gain_hbm,
    route_hbm,
    send_ref,
    normed_ref,
    tokens_ref,
    gain_ref,
    route_ref,
    sems,
    *,
    slots,
    pieces,
    experts,
):
    core = lax.axis_index("tp")
    loads = [
        pltpu.make_async_copy(src, dst, sems.at[i])
        for i, (src, dst) in enumerate(
            ((route_hbm, route_ref), (tokens_hbm, tokens_ref), (gain_hbm, gain_ref))
        )
    ]
    for load in loads:
        load.start()
    loads[0].wait()
    pick = chosen(route_ref[...], core, slots, pieces, experts).astype(BF16)
    loads[1].wait()
    loads[2].wait()
    values = tokens_ref[...].astype(F32)
    scaled = values * lax.rsqrt(jnp.mean(values * values, axis=-1, keepdims=True) + EPSILON)
    normed = (scaled * gain_ref[...].astype(F32)[None, :]).astype(BF16)
    normed_ref[...] = normed
    piece = normed.shape[1] // pieces
    stacked = jnp.concatenate([normed[:, q * piece : (q + 1) * piece] for q in range(pieces)], axis=0)
    send_ref[...] = jnp.dot(pick, stacked, preferred_element_type=F32).astype(BF16)


def gathering(half, pieces):
    to, frm = iota((half * pieces, half * pieces), 0), iota((half * pieces, half * pieces), 1)
    return jnp.where(frm == (to % half) * pieces + to // half, 1.0, 0.0).astype(BF16)


def expert_kernel(
    rows_ref,
    normed_ref,
    gate2_ref,
    up2_ref,
    down2_ref,
    gate_hbm,
    up_hbm,
    down_hbm,
    shared_gate_hbm,
    shared_up_hbm,
    shared_down_hbm,
    route_hbm,
    weight_hbm,
    out_ref,
    part_ref,
    mix_ref,
    gate_ref,
    up_ref,
    down_ref,
    shared_gate_ref,
    shared_up_ref,
    shared_down_ref,
    route_ref,
    weight_ref,
    sems,
    *,
    slots,
    pieces,
    experts,
):
    core = lax.axis_index("tp")
    loads = [
        pltpu.make_async_copy(src, dst, sems.at[i])
        for i, (src, dst) in enumerate(
            (
                (route_hbm, route_ref),
                (weight_hbm, weight_ref),
                (gate_hbm, gate_ref),
                (up_hbm, up_ref),
                (down_hbm, down_ref),
                (shared_gate_hbm, shared_gate_ref),
                (shared_up_hbm, shared_up_ref),
                (shared_down_hbm, shared_down_ref),
            )
        )
    ]
    for load in loads:
        load.start()
    total = rows_ref.shape[0]
    rows, block = total // pieces, total // 2
    half = rows // 2
    piece = rows_ref.shape[1]
    order = gathering(half, pieces)
    parts = [
        jnp.dot(order, rows_ref[h * block : (h + 1) * block, :], preferred_element_type=F32).astype(BF16)
        for h in range(2)
    ]
    inputs = jnp.concatenate(
        [
            jnp.concatenate([parts[h][q * half : (q + 1) * half] for h in range(2)], axis=0)
            for q in range(pieces)
        ],
        axis=1,
    )

    def swiglu(values, g, u):
        gate = jnp.dot(values, g[...], preferred_element_type=F32)
        upward = jnp.dot(values, u[...], preferred_element_type=F32)
        return (gate * jax.nn.sigmoid(gate) * upward).astype(BF16)

    hidden2 = swiglu(inputs, gate2_ref, up2_ref)
    loads[2].wait()
    loads[3].wait()
    hidden = swiglu(inputs, gate_ref, up_ref)
    back = order.T
    loads[4].wait()
    results = []
    for q in range(pieces):
        span = slice(q * piece, (q + 1) * piece)
        results.append(
            (
                jnp.dot(hidden2, down2_ref[:, span], preferred_element_type=F32)
                + jnp.dot(hidden, down_ref[:, span], preferred_element_type=F32)
            ).astype(BF16)
        )
    for h in range(2):
        lined = jnp.concatenate([r[h * half : (h + 1) * half] for r in results], axis=0)
        out_ref[h * block : (h + 1) * block, :] = jnp.dot(back, lined, preferred_element_type=F32).astype(BF16)

    for load in loads[:2] + loads[5:]:
        load.wait()
    normed = normed_ref[...]
    tokens = normed.shape[0]
    hidden = swiglu(normed, shared_gate_ref, shared_up_ref)
    for q in range(pieces):
        part_ref[q * tokens : (q + 1) * tokens, :] = jnp.dot(
            hidden, shared_down_ref[:, q * piece : (q + 1) * piece], preferred_element_type=F32
        )
    mix = chosen(route_ref[...], core, slots, pieces, experts, weight_ref[...]).T
    high = mix.astype(BF16)
    mix_ref[: mix.shape[0], :] = high
    mix_ref[mix.shape[0] :, :] = (mix - high.astype(F32)).astype(BF16)


def combine_kernel(mix_ref, returned_ref, part_ref, out_ref):
    both = jnp.dot(mix_ref[...], returned_ref[...], preferred_element_type=F32)
    size = both.shape[0] // 2
    out_ref[...] = part_ref[...] + both[:size] + both[size:]


def closing_kernel(mine_ref, other_ref, gain_ref, out_ref, total_ref, *, pieces):
    core = lax.axis_index("tp")
    total = mine_ref[...] + other_ref[...]
    total_ref[...] = total
    tokens, piece = total.shape[0] // pieces, total.shape[1]
    squares = jnp.sum(total * total, axis=1, keepdims=True)
    squares = functools.reduce(jnp.add, [squares[q * tokens : (q + 1) * tokens] for q in range(pieces)])
    scale = lax.rsqrt(squares / (pieces * piece) + EPSILON)
    mine = out_ref.shape[1] // piece
    gain = gain_ref[...].astype(F32)[None, :]
    for q in range(mine):
        start = pl.multiple_of((core * mine + q) * tokens, 8)
        values = total_ref[pl.ds(start, tokens), :] * scale
        out_ref[:, q * piece : (q + 1) * piece] = (values * gain[:, q * piece : (q + 1) * piece]).astype(BF16)


def body(
    tokens,
    in_gain,
    route_expert,
    route_weight,
    gate_weight,
    up_weight,
    down_weight,
    shared_gate,
    shared_up,
    shared_down,
    out_gain,
):
    experts, cores = lax.axis_size("ep"), lax.axis_size("tp")
    local_tokens, width = tokens.shape
    top_count = route_expert.shape[1]
    capacity = max(2, (local_tokens * top_count * 4 + 3 * experts - 1) // (3 * experts))
    slots = capacity // cores
    pieces = 8 // slots
    piece = width // pieces
    rows = experts * slots * pieces
    sizes = dict(slots=slots, pieces=pieces, experts=experts)

    swap = [(i, (i + 1) % cores) for i in range(cores)]
    weights = (gate_weight[0], up_weight[0], down_weight[0])
    others = tuple(lax.ppermute(w, "tp", swap) for w in weights)

    send, normed = pl.pallas_call(
        functools.partial(dispatch_kernel, **sizes),
        out_shape=(
            VMEM((rows, piece), BF16),
            VMEM((local_tokens, width), BF16),
        ),
        in_specs=[anywhere()] * 3,
        out_specs=(whole(), whole()),
        scratch_shapes=[
            VMEM(tokens.shape, BF16),
            VMEM(in_gain.shape, BF16),
            VMEM(route_expert.shape[::-1], jnp.int32),
            pltpu.SemaphoreType.DMA((3,)),
        ],
        compiler_params=grant(6),
        name="dispatch",
    )(*far(tokens, in_gain, route_expert.T))
    with jax.named_scope("outward"):
        arrived = lax.all_to_all(send.reshape(experts, slots * pieces, piece), "ep", 0, 0, tiled=True)

    loaded = (*weights, shared_gate, shared_up, shared_down, route_expert.T, route_weight.T)
    results, part, mix = pl.pallas_call(
        functools.partial(expert_kernel, **sizes),
        out_shape=(
            VMEM((rows, piece), BF16),
            VMEM((pieces * local_tokens, piece), F32),
            VMEM((2 * pieces * local_tokens, rows), BF16),
        ),
        in_specs=[whole()] * 5 + [anywhere()] * len(loaded),
        out_specs=(whole(),) * 3,
        scratch_shapes=[VMEM(w.shape, w.dtype) for w in loaded] + [pltpu.SemaphoreType.DMA((len(loaded),))],
        compiler_params=grant(20),
        name="expert",
    )(*held(arrived.reshape(rows, piece), normed, *others), *far(*loaded))
    with jax.named_scope("homeward"):
        returned = lax.all_to_all(results.reshape(experts, slots * pieces, piece), "ep", 0, 0, tiled=True)

    mine = pl.pallas_call(
        combine_kernel,
        out_shape=VMEM((pieces * local_tokens, piece), F32),
        in_specs=[whole()] * 3,
        out_specs=whole(),
        compiler_params=grant(4),
        name="combine",
    )(*held(mix, returned.reshape(rows, piece), part))
    other = lax.ppermute(mine, "tp", swap)
    return pl.pallas_call(
        functools.partial(closing_kernel, pieces=pieces),
        out_shape=jax.ShapeDtypeStruct((local_tokens, out_gain.shape[0]), BF16),
        in_specs=[whole()] * 3,
        out_specs=whole(),
        scratch_shapes=[VMEM((pieces * local_tokens, piece), F32)],
        compiler_params=grant(4),
        name="closing",
    )(*held(mine, other, out_gain))


def solution(mesh):
    return jax.shard_map(
        body,
        mesh=mesh,
        in_specs=(
            P(("grp", "ep"), None),
            P(),
            P(("grp", "ep"), None),
            P(("grp", "ep"), None),
            P("ep", None, "tp"),
            P("ep", None, "tp"),
            P("ep", "tp", None),
            P(None, "tp"),
            P(None, "tp"),
            P("tp", None),
            P("tp"),
        ),
        out_specs=P(("grp", "ep"), "tp"),
        check_vma=False,
    )
```

```python
import functools

import jax
import jax.numpy as jnp
from jax import lax
from jax.experimental import pallas as pl
from jax.experimental.pallas import tpu as pltpu
from jax.sharding import PartitionSpec as P


EPSILON = 1e-06
F32 = jnp.float32
BF16 = jnp.bfloat16
VMEM = pltpu.VMEM


def whole():
    return pl.BlockSpec(memory_space=VMEM)


def anywhere():
    return pl.BlockSpec(memory_space=pl.ANY)


def held(*arrays):
    return [pltpu.with_memory_space_constraint(a, VMEM) for a in arrays]


def far(*arrays):
    return [pltpu.with_memory_space_constraint(a, pltpu.HBM) for a in arrays]


def grant(mebibytes):
    return pltpu.CompilerParams(vmem_limit_bytes=mebibytes * 1024 * 1024)


def iota(shape, dim):
    return lax.broadcasted_iota(jnp.int32, shape, dim)


def chosen(route, core, slots, pieces, experts, values=None):
    top, tokens = route.shape
    rows, lanes = experts * slots * pieces, pieces * tokens
    row, lane = iota((rows, lanes), 0), iota((rows, lanes), 1)
    expert = row // (slots * pieces)
    tiled = jnp.concatenate([route] * pieces, axis=1)
    hits = [tiled[k : k + 1] == expert for k in range(top)]
    named = functools.reduce(jnp.logical_or, hits)
    before, after = iota((lanes, lanes), 0), iota((lanes, lanes), 1)
    earlier = (before // tokens == after // tokens) & (before < after)
    ones = jnp.where(named, 1.0, 0.0).astype(BF16)
    rank = jnp.dot(ones, jnp.where(earlier, 1.0, 0.0).astype(BF16), preferred_element_type=F32)
    wanted = ((row // pieces) % slots + slots * core).astype(F32)
    keep = named & (rank == wanted) & (lane // tokens == row % pieces)
    if values is None:
        return jnp.where(keep, 1.0, 0.0)
    spread = jnp.concatenate([values] * pieces, axis=1)
    total = jnp.zeros((rows, lanes), F32)
    for k in range(top):
        total = jnp.where(hits[k], spread[k : k + 1], total)
    return jnp.where(keep, total, 0.0)


def dispatch_kernel(
    tokens_hbm,
    gain_hbm,
    route_hbm,
    send_ref,
    normed_ref,
    tokens_ref,
    gain_ref,
    route_ref,
    sems,
    *,
    slots,
    pieces,
    experts,
):
    core = lax.axis_index("tp")
    loads = [
        pltpu.make_async_copy(src, dst, sems.at[i])
        for i, (src, dst) in enumerate(
            ((route_hbm, route_ref), (tokens_hbm, tokens_ref), (gain_hbm, gain_ref))
        )
    ]
    for load in loads:
        load.start()
    loads[0].wait()
    pick = chosen(route_ref[...], core, slots, pieces, experts).astype(BF16)
    loads[1].wait()
    loads[2].wait()
    values = tokens_ref[...].astype(F32)
    scaled = values * lax.rsqrt(jnp.mean(values * values, axis=-1, keepdims=True) + EPSILON)
    normed = (scaled * gain_ref[...].astype(F32)[None, :]).astype(BF16)
    normed_ref[...] = normed
    piece = normed.shape[1] // pieces
    stacked = jnp.concatenate([normed[:, q * piece : (q + 1) * piece] for q in range(pieces)], axis=0)
    send_ref[...] = jnp.dot(pick, stacked, preferred_element_type=F32).astype(BF16)


def gathering(half, pieces):
    to, frm = iota((half * pieces, half * pieces), 0), iota((half * pieces, half * pieces), 1)
    return jnp.where(frm == (to % half) * pieces + to // half, 1.0, 0.0).astype(BF16)


def swiglu(values, g, u):
    gate = jnp.dot(values, g[...], preferred_element_type=F32)
    upward = jnp.dot(values, u[...], preferred_element_type=F32)
    return (gate * jax.nn.sigmoid(gate) * upward).astype(BF16)


def side_kernel(
    normed_ref,
    shared_gate_hbm,
    shared_up_hbm,
    shared_down_hbm,
    route_hbm,
    weight_hbm,
    part_ref,
    mix_ref,
    shared_gate_ref,
    shared_up_ref,
    shared_down_ref,
    route_ref,
    weight_ref,
    sems,
    *,
    slots,
    pieces,
    experts,
):
    core = lax.axis_index("tp")
    pairs = (
        (route_hbm, route_ref),
        (weight_hbm, weight_ref),
        (shared_gate_hbm, shared_gate_ref),
        (shared_up_hbm, shared_up_ref),
        (shared_down_hbm, shared_down_ref),
    )
    loads = [pltpu.make_async_copy(src, dst, sems.at[i]) for i, (src, dst) in enumerate(pairs)]
    for load in loads:
        load.start()
    for load in loads[:2]:
        load.wait()
    mix = chosen(route_ref[...], core, slots, pieces, experts, weight_ref[...]).T
    high = mix.astype(BF16)
    mix_ref[: mix.shape[0], :] = high
    mix_ref[mix.shape[0] :, :] = (mix - high.astype(F32)).astype(BF16)
    for load in loads[2:]:
        load.wait()
    normed = normed_ref[...]
    tokens, piece = normed.shape[0], normed.shape[1] // pieces
    hidden = swiglu(normed, shared_gate_ref, shared_up_ref)
    for q in range(pieces):
        part_ref[q * tokens : (q + 1) * tokens, :] = jnp.dot(
            hidden, shared_down_ref[:, q * piece : (q + 1) * piece], preferred_element_type=F32
        )


def expert_kernel(
    rows_ref,
    gate2_ref,
    up2_hbm,
    gate_hbm,
    up_hbm,
    down2_hbm,
    down_hbm,
    out_ref,
    up2_ref,
    gate_ref,
    up_ref,
    down2_ref,
    down_ref,
    sems,
    *,
    pieces,
):
    pairs = (
        (up2_hbm, up2_ref),
        (gate_hbm, gate_ref),
        (up_hbm, up_ref),
        (down2_hbm, down2_ref),
        (down_hbm, down_ref),
    )
    loads = [pltpu.make_async_copy(src, dst, sems.at[i]) for i, (src, dst) in enumerate(pairs)]
    for load in loads:
        load.start()
    total = rows_ref.shape[0]
    rows, block = total // pieces, total // 2
    half = rows // 2
    piece = rows_ref.shape[1]
    order = gathering(half, pieces)
    parts = [
        jnp.dot(order, rows_ref[h * block : (h + 1) * block, :], preferred_element_type=F32).astype(BF16)
        for h in range(2)
    ]
    inputs = jnp.concatenate(
        [
            jnp.concatenate([parts[h][q * half : (q + 1) * half] for h in range(2)], axis=0)
            for q in range(pieces)
        ],
        axis=1,
    )
    loads[0].wait()
    hidden2 = swiglu(inputs, gate2_ref, up2_ref)
    loads[1].wait()
    loads[2].wait()
    hidden = swiglu(inputs, gate_ref, up_ref)
    loads[3].wait()
    loads[4].wait()
    back = order.T
    results = []
    for q in range(pieces):
        span = slice(q * piece, (q + 1) * piece)
        results.append(
            (
                jnp.dot(hidden, down_ref[:, span], preferred_element_type=F32)
                + jnp.dot(hidden2, down2_ref[:, span], preferred_element_type=F32)
            ).astype(BF16)
        )
    for h in range(2):
        lined = jnp.concatenate([r[h * half : (h + 1) * half] for r in results], axis=0)
        out_ref[h * block : (h + 1) * block, :] = jnp.dot(back, lined, preferred_element_type=F32).astype(BF16)


def combine_kernel(mix_ref, returned_ref, part_ref, out_ref):
    both = jnp.dot(mix_ref[...], returned_ref[...], preferred_element_type=F32)
    size = both.shape[0] // 2
    out_ref[...] = part_ref[...] + both[:size] + both[size:]


def closing_kernel(mine_ref, other_ref, gain_ref, out_ref, total_ref, *, pieces):
    core = lax.axis_index("tp")
    total = mine_ref[...] + other_ref[...]
    total_ref[...] = total
    tokens, piece = total.shape[0] // pieces, total.shape[1]
    squares = jnp.sum(total * total, axis=1, keepdims=True)
    squares = functools.reduce(jnp.add, [squares[q * tokens : (q + 1) * tokens] for q in range(pieces)])
    scale = lax.rsqrt(squares / (pieces * piece) + EPSILON)
    mine = out_ref.shape[1] // piece
    gain = gain_ref[...].astype(F32)[None, :]
    for q in range(mine):
        start = pl.multiple_of((core * mine + q) * tokens, 8)
        values = total_ref[pl.ds(start, tokens), :] * scale
        out_ref[:, q * piece : (q + 1) * piece] = (values * gain[:, q * piece : (q + 1) * piece]).astype(BF16)


def body(
    tokens,
    in_gain,
    route_expert,
    route_weight,
    gate_weight,
    up_weight,
    down_weight,
    shared_gate,
    shared_up,
    shared_down,
    out_gain,
):
    experts, cores = lax.axis_size("ep"), lax.axis_size("tp")
    local_tokens, width = tokens.shape
    top_count = route_expert.shape[1]
    capacity = max(2, (local_tokens * top_count * 4 + 3 * experts - 1) // (3 * experts))
    slots = capacity // cores
    pieces = 8 // slots
    piece = width // pieces
    rows = experts * slots * pieces
    sizes = dict(slots=slots, pieces=pieces, experts=experts)

    swap = [(i, (i + 1) % cores) for i in range(cores)]
    weights = (gate_weight[0], up_weight[0], down_weight[0])
    others = tuple(lax.ppermute(w, "tp", swap) for w in weights)

    send, normed = pl.pallas_call(
        functools.partial(dispatch_kernel, **sizes),
        out_shape=(
            VMEM((rows, piece), BF16),
            VMEM((local_tokens, width), BF16),
        ),
        in_specs=[anywhere()] * 3,
        out_specs=(whole(), whole()),
        scratch_shapes=[
            VMEM(tokens.shape, BF16),
            VMEM(in_gain.shape, BF16),
            VMEM(route_expert.shape[::-1], jnp.int32),
            pltpu.SemaphoreType.DMA((3,)),
        ],
        compiler_params=grant(6),
        name="dispatch",
    )(*far(tokens, in_gain, route_expert.T))
    arrived = lax.all_to_all(send.reshape(experts, slots * pieces, piece), "ep", 0, 0, tiled=True)

    loaded = (shared_gate, shared_up, shared_down, route_expert.T, route_weight.T)
    part, mix = pl.pallas_call(
        functools.partial(side_kernel, **sizes),
        out_shape=(
            VMEM((pieces * local_tokens, piece), F32),
            VMEM((2 * pieces * local_tokens, rows), BF16),
        ),
        in_specs=[whole()] + [anywhere()] * len(loaded),
        out_specs=(whole(), whole()),
        scratch_shapes=[VMEM(w.shape, w.dtype) for w in loaded] + [pltpu.SemaphoreType.DMA((len(loaded),))],
        compiler_params=grant(12),
        name="side",
    )(*held(normed), *far(*loaded))

    fetched = (others[1], weights[0], weights[1], others[2], weights[2])
    results = pl.pallas_call(
        functools.partial(expert_kernel, pieces=pieces),
        out_shape=VMEM((rows, piece), BF16),
        in_specs=[whole()] * 2 + [anywhere()] * len(fetched),
        out_specs=whole(),
        scratch_shapes=[VMEM(w.shape, w.dtype) for w in fetched] + [pltpu.SemaphoreType.DMA((len(fetched),))],
        compiler_params=grant(16),
        name="expert",
    )(*held(arrived.reshape(rows, piece), others[0]), *far(*fetched))
    returned = lax.all_to_all(results.reshape(experts, slots * pieces, piece), "ep", 0, 0, tiled=True)

    mine = pl.pallas_call(
        combine_kernel,
        out_shape=VMEM((pieces * local_tokens, piece), F32),
        in_specs=[whole()] * 3,
        out_specs=whole(),
        compiler_params=grant(4),
        name="combine",
    )(*held(mix, returned.reshape(rows, piece), part))
    other = lax.ppermute(mine, "tp", swap)
    return pl.pallas_call(
        functools.partial(closing_kernel, pieces=pieces),
        out_shape=jax.ShapeDtypeStruct((local_tokens, out_gain.shape[0]), BF16),
        in_specs=[whole()] * 3,
        out_specs=whole(),
        scratch_shapes=[VMEM((pieces * local_tokens, piece), F32)],
        compiler_params=grant(4),
        name="closing",
    )(*held(mine, other, out_gain))


def solution(mesh):
    return jax.shard_map(
        body,
        mesh=mesh,
        in_specs=(
            P(("grp", "ep"), None),
            P(),
            P(("grp", "ep"), None),
            P(("grp", "ep"), None),
            P("ep", None, "tp"),
            P("ep", None, "tp"),
            P("ep", "tp", None),
            P(None, "tp"),
            P(None, "tp"),
            P("tp", None),
            P("tp"),
        ),
        out_specs=P(("grp", "ep"), "tp"),
        check_vma=False,
    )
```

```python
import functools
import math

import jax
import jax.numpy as jnp
from jax import lax
from jax.experimental import pallas as pl
from jax.experimental.pallas import tpu as pltpu
from jax.sharding import PartitionSpec as P


EPSILON = 1e-06
F32 = jnp.float32
BF16 = jnp.bfloat16
VMEM = pltpu.VMEM


def whole():
    return pl.BlockSpec(memory_space=VMEM)


def anywhere():
    return pl.BlockSpec(memory_space=pl.ANY)


def held(*arrays):
    return [pltpu.with_memory_space_constraint(a, VMEM) for a in arrays]


def far(*arrays):
    return [pltpu.with_memory_space_constraint(a, pltpu.HBM) for a in arrays]


def grant(mebibytes):
    return pltpu.CompilerParams(vmem_limit_bytes=mebibytes * 1024 * 1024)


def iota(shape, dim):
    return lax.broadcasted_iota(jnp.int32, shape, dim)


def seated(block, experts):
    side = math.isqrt(experts)
    if side * side != experts or side % 2:
        return block

    def spread(i):
        return i // 2 + i % 2 * (side // 2)

    return experts - 1 - spread(block // side) * side - spread(block % side)


def chosen(route, core, slots, pieces, experts, values=None):
    top, tokens = route.shape
    rows, lanes = experts * slots * pieces, pieces * tokens
    row, lane = iota((rows, lanes), 0), iota((rows, lanes), 1)
    expert = seated(row // (slots * pieces), experts)
    tiled = jnp.concatenate([route] * pieces, axis=1)
    hits = [tiled[k : k + 1] == expert for k in range(top)]
    named = functools.reduce(jnp.logical_or, hits)
    before, after = iota((lanes, lanes), 0), iota((lanes, lanes), 1)
    earlier = (before // tokens == after // tokens) & (before < after)
    ones = jnp.where(named, 1.0, 0.0).astype(BF16)
    rank = jnp.dot(ones, jnp.where(earlier, 1.0, 0.0).astype(BF16), preferred_element_type=F32)
    wanted = ((row // pieces) % slots + slots * core).astype(F32)
    keep = named & (rank == wanted) & (lane // tokens == row % pieces)
    if values is None:
        return jnp.where(keep, 1.0, 0.0)
    spread = jnp.concatenate([values] * pieces, axis=1)
    total = jnp.zeros((rows, lanes), F32)
    for k in range(top):
        total = jnp.where(hits[k], spread[k : k + 1], total)
    return jnp.where(keep, total, 0.0)


def dispatch_kernel(
    tokens_hbm,
    gain_hbm,
    route_hbm,
    send_ref,
    normed_ref,
    tokens_ref,
    gain_ref,
    route_ref,
    sems,
    *,
    slots,
    pieces,
    experts,
):
    core = lax.axis_index("tp")
    loads = [
        pltpu.make_async_copy(src, dst, sems.at[i])
        for i, (src, dst) in enumerate(
            ((route_hbm, route_ref), (tokens_hbm, tokens_ref), (gain_hbm, gain_ref))
        )
    ]
    for load in loads:
        load.start()
    loads[0].wait()
    pick = chosen(route_ref[...], core, slots, pieces, experts).astype(BF16)
    loads[1].wait()
    loads[2].wait()
    values = tokens_ref[...].astype(F32)
    scaled = values * lax.rsqrt(jnp.mean(values * values, axis=-1, keepdims=True) + EPSILON)
    normed = (scaled * gain_ref[...].astype(F32)[None, :]).astype(BF16)
    normed_ref[...] = normed
    piece = normed.shape[1] // pieces
    stacked = jnp.concatenate([normed[:, q * piece : (q + 1) * piece] for q in range(pieces)], axis=0)
    send_ref[...] = jnp.dot(pick, stacked, preferred_element_type=F32).astype(BF16)


def gathering(half, pieces):
    to, frm = iota((half * pieces, half * pieces), 0), iota((half * pieces, half * pieces), 1)
    return jnp.where(frm == (to % half) * pieces + to // half, 1.0, 0.0).astype(BF16)


def swiglu(values, g, u):
    gate = jnp.dot(values, g[...], preferred_element_type=F32)
    upward = jnp.dot(values, u[...], preferred_element_type=F32)
    return (gate * jax.nn.sigmoid(gate) * upward).astype(BF16)


def side_kernel(
    normed_ref,
    shared_gate_hbm,
    shared_up_hbm,
    shared_down_hbm,
    route_hbm,
    weight_hbm,
    part_ref,
    mix_ref,
    shared_gate_ref,
    shared_up_ref,
    shared_down_ref,
    route_ref,
    weight_ref,
    sems,
    *,
    slots,
    pieces,
    experts,
):
    core = lax.axis_index("tp")
    pairs = (
        (route_hbm, route_ref),
        (weight_hbm, weight_ref),
        (shared_gate_hbm, shared_gate_ref),
        (shared_up_hbm, shared_up_ref),
        (shared_down_hbm, shared_down_ref),
    )
    loads = [pltpu.make_async_copy(src, dst, sems.at[i]) for i, (src, dst) in enumerate(pairs)]
    for load in loads:
        load.start()
    for load in loads[:2]:
        load.wait()
    mix = chosen(route_ref[...], core, slots, pieces, experts, weight_ref[...]).T
    high = mix.astype(BF16)
    mix_ref[: mix.shape[0], :] = high
    mix_ref[mix.shape[0] :, :] = (mix - high.astype(F32)).astype(BF16)
    for load in loads[2:]:
        load.wait()
    normed = normed_ref[...]
    tokens, piece = normed.shape[0], normed.shape[1] // pieces
    hidden = swiglu(normed, shared_gate_ref, shared_up_ref)
    for q in range(pieces):
        part_ref[q * tokens : (q + 1) * tokens, :] = jnp.dot(
            hidden, shared_down_ref[:, q * piece : (q + 1) * piece], preferred_element_type=F32
        )


def expert_kernel(
    rows_ref,
    gate2_ref,
    up2_hbm,
    gate_hbm,
    up_hbm,
    down2_hbm,
    down_hbm,
    out_ref,
    up2_ref,
    gate_ref,
    up_ref,
    down2_ref,
    down_ref,
    sems,
    *,
    pieces,
):
    pairs = (
        (up2_hbm, up2_ref),
        (gate_hbm, gate_ref),
        (up_hbm, up_ref),
        (down2_hbm, down2_ref),
        (down_hbm, down_ref),
    )
    loads = [pltpu.make_async_copy(src, dst, sems.at[i]) for i, (src, dst) in enumerate(pairs)]
    for load in loads:
        load.start()
    total = rows_ref.shape[0]
    rows, block = total // pieces, total // 2
    half = rows // 2
    piece = rows_ref.shape[1]
    order = gathering(half, pieces)
    parts = [
        jnp.dot(order, rows_ref[h * block : (h + 1) * block, :], preferred_element_type=F32).astype(BF16)
        for h in range(2)
    ]
    inputs = jnp.concatenate(
        [
            jnp.concatenate([parts[h][q * half : (q + 1) * half] for h in range(2)], axis=0)
            for q in range(pieces)
        ],
        axis=1,
    )
    loads[0].wait()
    hidden2 = swiglu(inputs, gate2_ref, up2_ref)
    loads[1].wait()
    loads[2].wait()
    hidden = swiglu(inputs, gate_ref, up_ref)
    loads[3].wait()
    loads[4].wait()
    back = order.T
    results = []
    for q in range(pieces):
        span = slice(q * piece, (q + 1) * piece)
        results.append(
            (
                jnp.dot(hidden, down_ref[:, span], preferred_element_type=F32)
                + jnp.dot(hidden2, down2_ref[:, span], preferred_element_type=F32)
            ).astype(BF16)
        )
    for h in range(2):
        lined = jnp.concatenate([r[h * half : (h + 1) * half] for r in results], axis=0)
        out_ref[h * block : (h + 1) * block, :] = jnp.dot(back, lined, preferred_element_type=F32).astype(BF16)


def combine_kernel(mix_ref, returned_ref, part_ref, out_ref):
    both = jnp.dot(mix_ref[...], returned_ref[...], preferred_element_type=F32)
    size = both.shape[0] // 2
    out_ref[...] = part_ref[...] + both[:size] + both[size:]


def closing_kernel(mine_ref, other_ref, gain_ref, out_ref, total_ref, *, pieces):
    core = lax.axis_index("tp")
    total = mine_ref[...] + other_ref[...]
    total_ref[...] = total
    tokens, piece = total.shape[0] // pieces, total.shape[1]
    squares = jnp.sum(total * total, axis=1, keepdims=True)
    squares = functools.reduce(jnp.add, [squares[q * tokens : (q + 1) * tokens] for q in range(pieces)])
    scale = lax.rsqrt(squares / (pieces * piece) + EPSILON)
    mine = out_ref.shape[1] // piece
    gain = gain_ref[...].astype(F32)[None, :]
    for q in range(mine):
        start = pl.multiple_of((core * mine + q) * tokens, 8)
        values = total_ref[pl.ds(start, tokens), :] * scale
        out_ref[:, q * piece : (q + 1) * piece] = (values * gain[:, q * piece : (q + 1) * piece]).astype(BF16)


def body(
    tokens,
    in_gain,
    route_expert,
    route_weight,
    gate_weight,
    up_weight,
    down_weight,
    shared_gate,
    shared_up,
    shared_down,
    out_gain,
):
    experts, cores = lax.axis_size("ep"), lax.axis_size("tp")
    local_tokens, width = tokens.shape
    top_count = route_expert.shape[1]
    capacity = max(2, (local_tokens * top_count * 4 + 3 * experts - 1) // (3 * experts))
    slots = capacity // cores
    pieces = 8 // slots
    piece = width // pieces
    rows = experts * slots * pieces
    sizes = dict(slots=slots, pieces=pieces, experts=experts)

    order = [[seated(block, experts) for block in range(experts)]]
    exchange = functools.partial(
        lax.all_to_all, axis_name="ep", split_axis=0, concat_axis=0, axis_index_groups=order, tiled=True
    )
    swap = [(i, (i + 1) % cores) for i in range(cores)]
    weights = (gate_weight[0], up_weight[0], down_weight[0])
    others = tuple(lax.ppermute(w, "tp", swap) for w in weights)

    send, normed = pl.pallas_call(
        functools.partial(dispatch_kernel, **sizes),
        out_shape=(
            VMEM((rows, piece), BF16),
            VMEM((local_tokens, width), BF16),
        ),
        in_specs=[anywhere()] * 3,
        out_specs=(whole(), whole()),
        scratch_shapes=[
            VMEM(tokens.shape, BF16),
            VMEM(in_gain.shape, BF16),
            VMEM(route_expert.shape[::-1], jnp.int32),
            pltpu.SemaphoreType.DMA((3,)),
        ],
        compiler_params=grant(6),
        name="dispatch",
    )(*far(tokens, in_gain, route_expert.T))
    arrived = exchange(send.reshape(experts, slots * pieces, piece))

    loaded = (shared_gate, shared_up, shared_down, route_expert.T, route_weight.T)
    part, mix = pl.pallas_call(
        functools.partial(side_kernel, **sizes),
        out_shape=(
            VMEM((pieces * local_tokens, piece), F32),
            VMEM((2 * pieces * local_tokens, rows), BF16),
        ),
        in_specs=[whole()] + [anywhere()] * len(loaded),
        out_specs=(whole(), whole()),
        scratch_shapes=[VMEM(w.shape, w.dtype) for w in loaded] + [pltpu.SemaphoreType.DMA((len(loaded),))],
        compiler_params=grant(12),
        name="side",
    )(*held(normed), *far(*loaded))

    fetched = (others[1], weights[0], weights[1], others[2], weights[2])
    results = pl.pallas_call(
        functools.partial(expert_kernel, pieces=pieces),
        out_shape=VMEM((rows, piece), BF16),
        in_specs=[whole()] * 2 + [anywhere()] * len(fetched),
        out_specs=whole(),
        scratch_shapes=[VMEM(w.shape, w.dtype) for w in fetched] + [pltpu.SemaphoreType.DMA((len(fetched),))],
        compiler_params=grant(16),
        name="expert",
    )(*held(arrived.reshape(rows, piece), others[0]), *far(*fetched))
    returned = exchange(results.reshape(experts, slots * pieces, piece))

    mine = pl.pallas_call(
        combine_kernel,
        out_shape=VMEM((pieces * local_tokens, piece), F32),
        in_specs=[whole()] * 3,
        out_specs=whole(),
        compiler_params=grant(4),
        name="combine",
    )(*held(mix, returned.reshape(rows, piece), part))
    other = lax.ppermute(mine, "tp", swap)
    return pl.pallas_call(
        functools.partial(closing_kernel, pieces=pieces),
        out_shape=jax.ShapeDtypeStruct((local_tokens, out_gain.shape[0]), BF16),
        in_specs=[whole()] * 3,
        out_specs=whole(),
        scratch_shapes=[VMEM((pieces * local_tokens, piece), F32)],
        compiler_params=grant(4),
        name="closing",
    )(*held(mine, other, out_gain))


def solution(mesh):
    return jax.shard_map(
        body,
        mesh=mesh,
        in_specs=(
            P(("grp", "ep"), None),
            P(),
            P(("grp", "ep"), None),
            P(("grp", "ep"), None),
            P("ep", None, "tp"),
            P("ep", None, "tp"),
            P("ep", "tp", None),
            P(None, "tp"),
            P(None, "tp"),
            P("tp", None),
            P("tp"),
        ),
        out_specs=P(("grp", "ep"), "tp"),
        check_vma=False,
    )
```

```python
import functools
import math

import jax
import jax.numpy as jnp
from jax import lax
from jax.experimental import pallas as pl
from jax.experimental.pallas import tpu as pltpu
from jax.sharding import PartitionSpec as P


EPSILON = 1e-06
F32 = jnp.float32
BF16 = jnp.bfloat16
VMEM = pltpu.VMEM


def whole():
    return pl.BlockSpec(memory_space=VMEM)


def anywhere():
    return pl.BlockSpec(memory_space=pl.ANY)


def held(*arrays):
    return [pltpu.with_memory_space_constraint(a, VMEM) for a in arrays]


def far(*arrays):
    return [pltpu.with_memory_space_constraint(a, pltpu.HBM) for a in arrays]


def grant(mebibytes):
    return pltpu.CompilerParams(vmem_limit_bytes=mebibytes * 1024 * 1024)


def iota(shape, dim):
    return lax.broadcasted_iota(jnp.int32, shape, dim)


def seated(block, experts):
    side = math.isqrt(experts)
    if side * side != experts or side % 2:
        return block

    def spread(i):
        return i // 2 + i % 2 * (side // 2)

    return experts - 1 - spread(block // side) * side - spread(block % side)


def chosen(route, core, slots, pieces, experts, values=None):
    top, tokens = route.shape
    rows, lanes = experts * slots * pieces, pieces * tokens
    row, lane = iota((rows, lanes), 0), iota((rows, lanes), 1)
    expert = seated(row // (slots * pieces), experts)
    tiled = jnp.concatenate([route] * pieces, axis=1)
    hits = [tiled[k : k + 1] == expert for k in range(top)]
    named = functools.reduce(jnp.logical_or, hits)
    before, after = iota((lanes, lanes), 0), iota((lanes, lanes), 1)
    earlier = (before // tokens == after // tokens) & (before < after)
    ones = jnp.where(named, 1.0, 0.0).astype(BF16)
    rank = jnp.dot(ones, jnp.where(earlier, 1.0, 0.0).astype(BF16), preferred_element_type=F32)
    wanted = ((row // pieces) % slots + slots * core).astype(F32)
    keep = named & (rank == wanted) & (lane // tokens == row % pieces)
    if values is None:
        return jnp.where(keep, 1.0, 0.0)
    spread = jnp.concatenate([values] * pieces, axis=1)
    total = jnp.zeros((rows, lanes), F32)
    for k in range(top):
        total = jnp.where(hits[k], spread[k : k + 1], total)
    return jnp.where(keep, total, 0.0)


def dispatch_kernel(
    tokens_hbm,
    gain_hbm,
    route_hbm,
    send_hbm,
    normed_ref,
    tokens_ref,
    gain_ref,
    route_ref,
    send_ref,
    sems,
    out_sems,
    *,
    slots,
    pieces,
    experts,
):
    core = lax.axis_index("tp")
    loads = [
        pltpu.make_async_copy(src, dst, sems.at[i])
        for i, (src, dst) in enumerate(
            ((route_hbm, route_ref), (tokens_hbm, tokens_ref), (gain_hbm, gain_ref))
        )
    ]
    for load in loads:
        load.start()
    loads[0].wait()
    pick = chosen(route_ref[...], core, slots, pieces, experts).astype(BF16)
    loads[1].wait()
    loads[2].wait()
    values = tokens_ref[...].astype(F32)
    scaled = values * lax.rsqrt(jnp.mean(values * values, axis=-1, keepdims=True) + EPSILON)
    normed = (scaled * gain_ref[...].astype(F32)[None, :]).astype(BF16)
    normed_ref[...] = normed
    piece = normed.shape[1] // pieces
    stacked = jnp.concatenate([normed[:, q * piece : (q + 1) * piece] for q in range(pieces)], axis=0)
    chunk = send_ref.shape[0] // 4
    stores = []
    for c in range(4):
        span = slice(c * chunk, (c + 1) * chunk)
        send_ref[span, :] = jnp.dot(pick[span], stacked, preferred_element_type=F32).astype(BF16)
        stores.append(
            pltpu.make_async_copy(
                send_ref.at[pl.ds(c * chunk, chunk)], send_hbm.at[pl.ds(c * chunk, chunk)], out_sems.at[c]
            )
        )
        stores[-1].start()
    for store in stores:
        store.wait()


def gathering(half, pieces):
    to, frm = iota((half * pieces, half * pieces), 0), iota((half * pieces, half * pieces), 1)
    return jnp.where(frm == (to % half) * pieces + to // half, 1.0, 0.0).astype(BF16)


def swiglu(values, g, u):
    gate = jnp.dot(values, g[...], preferred_element_type=F32)
    upward = jnp.dot(values, u[...], preferred_element_type=F32)
    return (gate * jax.nn.sigmoid(gate) * upward).astype(BF16)


def side_kernel(
    normed_ref,
    shared_gate_hbm,
    shared_up_hbm,
    shared_down_hbm,
    route_hbm,
    weight_hbm,
    part_ref,
    mix_ref,
    shared_gate_ref,
    shared_up_ref,
    shared_down_ref,
    route_ref,
    weight_ref,
    sems,
    *,
    slots,
    pieces,
    experts,
):
    core = lax.axis_index("tp")
    pairs = (
        (route_hbm, route_ref),
        (weight_hbm, weight_ref),
        (shared_gate_hbm, shared_gate_ref),
        (shared_up_hbm, shared_up_ref),
        (shared_down_hbm, shared_down_ref),
    )
    loads = [pltpu.make_async_copy(src, dst, sems.at[i]) for i, (src, dst) in enumerate(pairs)]
    for load in loads:
        load.start()
    for load in loads[:2]:
        load.wait()
    mix = chosen(route_ref[...], core, slots, pieces, experts, weight_ref[...]).T
    high = mix.astype(BF16)
    mix_ref[: mix.shape[0], :] = high
    mix_ref[mix.shape[0] :, :] = (mix - high.astype(F32)).astype(BF16)
    for load in loads[2:]:
        load.wait()
    normed = normed_ref[...]
    tokens, piece = normed.shape[0], normed.shape[1] // pieces
    hidden = swiglu(normed, shared_gate_ref, shared_up_ref)
    for q in range(pieces):
        part_ref[q * tokens : (q + 1) * tokens, :] = jnp.dot(
            hidden, shared_down_ref[:, q * piece : (q + 1) * piece], preferred_element_type=F32
        )


def opening_kernel(
    rows_ref, gate_hbm, up_hbm, down_hbm, inputs_ref, hidden_ref, down_ref, gate_ref, up_ref, sems, *, pieces
):
    pairs = ((gate_hbm, gate_ref), (up_hbm, up_ref), (down_hbm, down_ref))
    loads = [pltpu.make_async_copy(src, dst, sems.at[i]) for i, (src, dst) in enumerate(pairs)]
    for load in loads:
        load.start()
    total = rows_ref.shape[0]
    block, half = total // 2, total // pieces // 2
    piece = rows_ref.shape[1]
    order = gathering(half, pieces)
    for h in range(2):
        part = jnp.dot(order, rows_ref[h * block : (h + 1) * block, :], preferred_element_type=F32).astype(BF16)
        for q in range(pieces):
            inputs_ref[h * half : (h + 1) * half, q * piece : (q + 1) * piece] = part[q * half : (q + 1) * half]
    inputs = inputs_ref[...]
    loads[0].wait()
    gate = jnp.dot(inputs, gate_ref[...], preferred_element_type=F32)
    loads[1].wait()
    upward = jnp.dot(inputs, up_ref[...], preferred_element_type=F32)
    hidden_ref[...] = (gate * jax.nn.sigmoid(gate) * upward).astype(BF16)
    loads[2].wait()


def expert_kernel(
    inputs_ref,
    hidden_ref,
    down_ref,
    gate2_ref,
    up2_hbm,
    down2_hbm,
    out_ref,
    up2_ref,
    down2_ref,
    sems,
    *,
    pieces,
):
    pairs = ((up2_hbm, up2_ref), (down2_hbm, down2_ref))
    loads = [pltpu.make_async_copy(src, dst, sems.at[i]) for i, (src, dst) in enumerate(pairs)]
    for load in loads:
        load.start()
    total, piece = out_ref.shape
    block, half = total // 2, total // pieces // 2
    inputs = inputs_ref[...]
    gate = jnp.dot(inputs, gate2_ref[...], preferred_element_type=F32)
    firsts = jnp.dot(hidden_ref[...], down_ref[...], preferred_element_type=F32)
    back = gathering(half, pieces).T
    loads[0].wait()
    upward = jnp.dot(inputs, up2_ref[...], preferred_element_type=F32)
    hidden2 = (gate * jax.nn.sigmoid(gate) * upward).astype(BF16)
    loads[1].wait()
    results = []
    for q in range(pieces):
        span = slice(q * piece, (q + 1) * piece)
        results.append(
            (
                firsts[:, span] + jnp.dot(hidden2, down2_ref[:, span], preferred_element_type=F32)
            ).astype(BF16)
        )
    for h in range(2):
        lined = jnp.concatenate([r[h * half : (h + 1) * half] for r in results], axis=0)
        out_ref[h * block : (h + 1) * block, :] = jnp.dot(back, lined, preferred_element_type=F32).astype(BF16)


def combine_kernel(mix_ref, returned_ref, part_ref, out_ref):
    both = jnp.dot(mix_ref[...], returned_ref[...], preferred_element_type=F32)
    size = both.shape[0] // 2
    out_ref[...] = part_ref[...] + both[:size] + both[size:]


def closing_kernel(mine_ref, other_ref, gain_ref, out_ref, total_ref, *, pieces):
    core = lax.axis_index("tp")
    total = mine_ref[...] + other_ref[...]
    total_ref[...] = total
    tokens, piece = total.shape[0] // pieces, total.shape[1]
    squares = jnp.sum(total * total, axis=1, keepdims=True)
    squares = functools.reduce(jnp.add, [squares[q * tokens : (q + 1) * tokens] for q in range(pieces)])
    scale = lax.rsqrt(squares / (pieces * piece) + EPSILON)
    mine = out_ref.shape[1] // piece
    gain = gain_ref[...].astype(F32)[None, :]
    for q in range(mine):
        start = pl.multiple_of((core * mine + q) * tokens, 8)
        values = total_ref[pl.ds(start, tokens), :] * scale
        out_ref[:, q * piece : (q + 1) * piece] = (values * gain[:, q * piece : (q + 1) * piece]).astype(BF16)


def body(
    tokens,
    in_gain,
    route_expert,
    route_weight,
    gate_weight,
    up_weight,
    down_weight,
    shared_gate,
    shared_up,
    shared_down,
    out_gain,
):
    experts, cores = lax.axis_size("ep"), lax.axis_size("tp")
    local_tokens, width = tokens.shape
    top_count = route_expert.shape[1]
    capacity = max(2, (local_tokens * top_count * 4 + 3 * experts - 1) // (3 * experts))
    slots = capacity // cores
    pieces = 8 // slots
    piece = width // pieces
    rows = experts * slots * pieces
    sizes = dict(slots=slots, pieces=pieces, experts=experts)

    order = [[seated(block, experts) for block in range(experts)]]
    exchange = functools.partial(
        lax.all_to_all, axis_name="ep", split_axis=0, concat_axis=0, axis_index_groups=order, tiled=True
    )
    swap = [(i, (i + 1) % cores) for i in range(cores)]
    weights = (gate_weight[0], up_weight[0], down_weight[0])
    others = tuple(lax.ppermute(w, "tp", swap) for w in weights)

    send, normed = pl.pallas_call(
        functools.partial(dispatch_kernel, **sizes),
        out_shape=(
            pltpu.HBM((rows, piece), BF16),
            VMEM((local_tokens, width), BF16),
        ),
        in_specs=[anywhere()] * 3,
        out_specs=(anywhere(), whole()),
        scratch_shapes=[
            VMEM(tokens.shape, BF16),
            VMEM(in_gain.shape, BF16),
            VMEM(route_expert.shape[::-1], jnp.int32),
            VMEM((rows, piece), BF16),
            pltpu.SemaphoreType.DMA((3,)),
            pltpu.SemaphoreType.DMA((4,)),
        ],
        compiler_params=grant(6),
        name="dispatch",
    )(*far(tokens, in_gain, route_expert.T))
    arrived = exchange(send.reshape(experts, slots * pieces, piece))

    loaded = (shared_gate, shared_up, shared_down, route_expert.T, route_weight.T)
    part, mix = pl.pallas_call(
        functools.partial(side_kernel, **sizes),
        out_shape=(
            VMEM((pieces * local_tokens, piece), F32),
            VMEM((2 * pieces * local_tokens, rows), BF16),
        ),
        in_specs=[whole()] + [anywhere()] * len(loaded),
        out_specs=(whole(), whole()),
        scratch_shapes=[VMEM(w.shape, w.dtype) for w in loaded] + [pltpu.SemaphoreType.DMA((len(loaded),))],
        compiler_params=grant(12),
        name="side",
    )(*held(normed), *far(*loaded))

    inputs, hidden, down = pl.pallas_call(
        functools.partial(opening_kernel, pieces=pieces),
        out_shape=(
            VMEM((rows // pieces, width), BF16),
            VMEM((rows // pieces, weights[0].shape[1]), BF16),
            VMEM(weights[2].shape, BF16),
        ),
        in_specs=[whole()] + [anywhere()] * 3,
        out_specs=(whole(),) * 3,
        scratch_shapes=[VMEM(w.shape, BF16) for w in weights[:2]] + [pltpu.SemaphoreType.DMA((3,))],
        compiler_params=grant(8),
        name="opening",
    )(*held(arrived.reshape(rows, piece)), *far(*weights))

    fetched = (others[1], others[2])
    results = pl.pallas_call(
        functools.partial(expert_kernel, pieces=pieces),
        out_shape=VMEM((rows, piece), BF16),
        in_specs=[whole()] * 4 + [anywhere()] * len(fetched),
        out_specs=whole(),
        scratch_shapes=[VMEM(w.shape, w.dtype) for w in fetched] + [pltpu.SemaphoreType.DMA((len(fetched),))],
        compiler_params=grant(12),
        name="expert",
    )(*held(inputs, hidden, down, others[0]), *far(*fetched))
    returned = exchange(results.reshape(experts, slots * pieces, piece))

    mine = pl.pallas_call(
        combine_kernel,
        out_shape=VMEM((pieces * local_tokens, piece), F32),
        in_specs=[whole()] * 3,
        out_specs=whole(),
        compiler_params=grant(4),
        name="combine",
    )(*held(mix, returned.reshape(rows, piece), part))
    other = lax.ppermute(mine, "tp", swap)
    return pl.pallas_call(
        functools.partial(closing_kernel, pieces=pieces),
        out_shape=jax.ShapeDtypeStruct((local_tokens, out_gain.shape[0]), BF16),
        in_specs=[whole()] * 3,
        out_specs=whole(),
        scratch_shapes=[VMEM((pieces * local_tokens, piece), F32)],
        compiler_params=grant(4),
        name="closing",
    )(*held(mine, other, out_gain))


def solution(mesh):
    return jax.shard_map(
        body,
        mesh=mesh,
        in_specs=(
            P(("grp", "ep"), None),
            P(),
            P(("grp", "ep"), None),
            P(("grp", "ep"), None),
            P("ep", None, "tp"),
            P("ep", None, "tp"),
            P("ep", "tp", None),
            P(None, "tp"),
            P(None, "tp"),
            P("tp", None),
            P("tp"),
        ),
        out_specs=P(("grp", "ep"), "tp"),
        check_vma=False,
    )
```

```python
import functools
import math

import jax
import jax.numpy as jnp
from jax import lax
from jax.experimental import pallas as pl
from jax.experimental.pallas import tpu as pltpu
from jax.sharding import PartitionSpec as P


EPSILON = 1e-06
F32 = jnp.float32
BF16 = jnp.bfloat16
VMEM = pltpu.VMEM


def whole():
    return pl.BlockSpec(memory_space=VMEM)


def anywhere():
    return pl.BlockSpec(memory_space=pl.ANY)


def held(*arrays):
    return [pltpu.with_memory_space_constraint(a, VMEM) for a in arrays]


def far(*arrays):
    return [pltpu.with_memory_space_constraint(a, pltpu.HBM) for a in arrays]


def grant(mebibytes):
    return pltpu.CompilerParams(vmem_limit_bytes=mebibytes * 1024 * 1024)


def iota(shape, dim):
    return lax.broadcasted_iota(jnp.int32, shape, dim)


def seated(block, experts):
    side = math.isqrt(experts)
    if side * side != experts or side % 2:
        return block

    def spread(i):
        return i // 2 + i % 2 * (side // 2)

    return experts - 1 - spread(block // side) * side - spread(block % side)


def chosen(route, core, slots, pieces, experts, values=None):
    top, tokens = route.shape
    rows, lanes = experts * slots * pieces, pieces * tokens
    row, lane = iota((rows, lanes), 0), iota((rows, lanes), 1)
    expert = seated(row // (slots * pieces), experts)
    tiled = jnp.concatenate([route] * pieces, axis=1)
    hits = [tiled[k : k + 1] == expert for k in range(top)]
    named = functools.reduce(jnp.logical_or, hits)
    before, after = iota((lanes, lanes), 0), iota((lanes, lanes), 1)
    earlier = (before // tokens == after // tokens) & (before < after)
    ones = jnp.where(named, 1.0, 0.0).astype(BF16)
    rank = jnp.dot(ones, jnp.where(earlier, 1.0, 0.0).astype(BF16), preferred_element_type=F32)
    wanted = ((row // pieces) % slots + slots * core).astype(F32)
    keep = named & (rank == wanted) & (lane // tokens == row % pieces)
    if values is None:
        return jnp.where(keep, 1.0, 0.0)
    spread = jnp.concatenate([values] * pieces, axis=1)
    total = jnp.zeros((rows, lanes), F32)
    for k in range(top):
        total = jnp.where(hits[k], spread[k : k + 1], total)
    return jnp.where(keep, total, 0.0)


def dispatch_kernel(
    tokens_hbm,
    gain_hbm,
    route_hbm,
    send_hbm,
    normed_ref,
    tokens_ref,
    gain_ref,
    route_ref,
    send_ref,
    sems,
    out_sems,
    *,
    slots,
    pieces,
    experts,
):
    core = lax.axis_index("tp")
    loads = [
        pltpu.make_async_copy(src, dst, sems.at[i])
        for i, (src, dst) in enumerate(
            ((route_hbm, route_ref), (tokens_hbm, tokens_ref), (gain_hbm, gain_ref))
        )
    ]
    for load in loads:
        load.start()
    for load in loads:
        load.wait()
    pick = chosen(route_ref[...], core, slots, pieces, experts).astype(BF16)
    values = tokens_ref[...].astype(F32)
    scaled = values * lax.rsqrt(jnp.mean(values * values, axis=-1, keepdims=True) + EPSILON)
    normed = (scaled * gain_ref[...].astype(F32)[None, :]).astype(BF16)
    normed_ref[...] = normed
    piece = normed.shape[1] // pieces
    stacked = jnp.concatenate([normed[:, q * piece : (q + 1) * piece] for q in range(pieces)], axis=0)
    chunk = send_ref.shape[0] // 4
    stores = []
    for c in range(4):
        span = slice(c * chunk, (c + 1) * chunk)
        send_ref[span, :] = jnp.dot(pick[span], stacked, preferred_element_type=F32).astype(BF16)
        stores.append(
            pltpu.make_async_copy(
                send_ref.at[pl.ds(c * chunk, chunk)], send_hbm.at[pl.ds(c * chunk, chunk)], out_sems.at[c]
            )
        )
        stores[-1].start()
    for store in stores:
        store.wait()


def gathering(half, pieces):
    to, frm = iota((half * pieces, half * pieces), 0), iota((half * pieces, half * pieces), 1)
    return jnp.where(frm == (to % half) * pieces + to // half, 1.0, 0.0).astype(BF16)


def side_kernel(
    normed_ref,
    shared_gate_hbm,
    shared_up_hbm,
    shared_down_hbm,
    route_hbm,
    weight_hbm,
    part_ref,
    mix_ref,
    shared_gate_ref,
    shared_up_ref,
    shared_down_ref,
    route_ref,
    weight_ref,
    sems,
    *,
    slots,
    pieces,
    experts,
):
    core = lax.axis_index("tp")
    pairs = (
        (route_hbm, route_ref),
        (weight_hbm, weight_ref),
        (shared_gate_hbm, shared_gate_ref),
        (shared_up_hbm, shared_up_ref),
        (shared_down_hbm, shared_down_ref),
    )
    loads = [pltpu.make_async_copy(src, dst, sems.at[i]) for i, (src, dst) in enumerate(pairs)]
    for load in loads:
        load.start()
    for load in loads[:2]:
        load.wait()
    mix = chosen(route_ref[...], core, slots, pieces, experts, weight_ref[...]).T
    high = mix.astype(BF16)
    mix_ref[: mix.shape[0], :] = high
    mix_ref[mix.shape[0] :, :] = (mix - high.astype(F32)).astype(BF16)
    normed = normed_ref[...]
    tokens, piece = normed.shape[0], normed.shape[1] // pieces
    loads[2].wait()
    gate = jnp.dot(normed, shared_gate_ref[...], preferred_element_type=F32)
    loads[3].wait()
    upward = jnp.dot(normed, shared_up_ref[...], preferred_element_type=F32)
    hidden = (gate * jax.nn.sigmoid(gate) * upward).astype(BF16)
    loads[4].wait()
    for q in range(pieces):
        part_ref[q * tokens : (q + 1) * tokens, :] = jnp.dot(
            hidden, shared_down_ref[:, q * piece : (q + 1) * piece], preferred_element_type=F32
        )


def opening_kernel(
    rows_ref, gate_hbm, up_hbm, down_hbm, inputs_ref, hidden_ref, down_ref, gate_ref, up_ref, sems, *, pieces
):
    pairs = ((gate_hbm, gate_ref), (up_hbm, up_ref), (down_hbm, down_ref))
    loads = [pltpu.make_async_copy(src, dst, sems.at[i]) for i, (src, dst) in enumerate(pairs)]
    for load in loads:
        load.start()
    total = rows_ref.shape[0]
    block, half = total // 2, total // pieces // 2
    piece = rows_ref.shape[1]
    order = gathering(half, pieces)
    for h in range(2):
        part = jnp.dot(order, rows_ref[h * block : (h + 1) * block, :], preferred_element_type=F32).astype(BF16)
        for q in range(pieces):
            inputs_ref[h * half : (h + 1) * half, q * piece : (q + 1) * piece] = part[q * half : (q + 1) * half]
    inputs = inputs_ref[...]
    loads[0].wait()
    gate = jnp.dot(inputs, gate_ref[...], preferred_element_type=F32)
    loads[1].wait()
    upward = jnp.dot(inputs, up_ref[...], preferred_element_type=F32)
    hidden_ref[...] = (gate * jax.nn.sigmoid(gate) * upward).astype(BF16)
    loads[2].wait()


def middle_kernel(
    inputs_ref, hidden_ref, down_ref, gate2_hbm, up2_hbm, hidden2_ref, first_ref, gate2_ref, up2_ref, sems
):
    pairs = ((gate2_hbm, gate2_ref), (up2_hbm, up2_ref))
    loads = [pltpu.make_async_copy(src, dst, sems.at[i]) for i, (src, dst) in enumerate(pairs)]
    for load in loads:
        load.start()
    first_ref[...] = jnp.dot(hidden_ref[...], down_ref[...], preferred_element_type=F32)
    inputs = inputs_ref[...]
    loads[0].wait()
    gate = jnp.dot(inputs, gate2_ref[...], preferred_element_type=F32)
    loads[1].wait()
    upward = jnp.dot(inputs, up2_ref[...], preferred_element_type=F32)
    hidden2_ref[...] = (gate * jax.nn.sigmoid(gate) * upward).astype(BF16)


def expert_kernel(hidden2_ref, first_ref, down2_ref, out_ref, *, pieces):
    total, piece = out_ref.shape
    block, half = total // 2, total // pieces // 2
    back = gathering(half, pieces).T
    hidden2 = hidden2_ref[...]
    results = []
    for q in range(pieces):
        span = slice(q * piece, (q + 1) * piece)
        results.append(
            (
                first_ref[:, span] + jnp.dot(hidden2, down2_ref[:, span], preferred_element_type=F32)
            ).astype(BF16)
        )
    for h in range(2):
        lined = jnp.concatenate([r[h * half : (h + 1) * half] for r in results], axis=0)
        out_ref[h * block : (h + 1) * block, :] = jnp.dot(back, lined, preferred_element_type=F32).astype(BF16)


def combine_kernel(mix_ref, returned_ref, part_ref, out_ref):
    both = jnp.dot(mix_ref[...], returned_ref[...], preferred_element_type=F32)
    size = both.shape[0] // 2
    out_ref[...] = part_ref[...] + both[:size] + both[size:]


def closing_kernel(mine_ref, other_ref, gain_ref, out_ref, total_ref, *, pieces):
    core = lax.axis_index("tp")
    total = mine_ref[...] + other_ref[...]
    total_ref[...] = total
    tokens, piece = total.shape[0] // pieces, total.shape[1]
    squares = jnp.sum(total * total, axis=1, keepdims=True)
    squares = functools.reduce(jnp.add, [squares[q * tokens : (q + 1) * tokens] for q in range(pieces)])
    scale = lax.rsqrt(squares / (pieces * piece) + EPSILON)
    mine = out_ref.shape[1] // piece
    gain = gain_ref[...].astype(F32)[None, :]
    for q in range(mine):
        start = pl.multiple_of((core * mine + q) * tokens, 8)
        values = total_ref[pl.ds(start, tokens), :] * scale
        out_ref[:, q * piece : (q + 1) * piece] = (values * gain[:, q * piece : (q + 1) * piece]).astype(BF16)


def body(
    tokens,
    in_gain,
    route_expert,
    route_weight,
    gate_weight,
    up_weight,
    down_weight,
    shared_gate,
    shared_up,
    shared_down,
    out_gain,
):
    experts, cores = lax.axis_size("ep"), lax.axis_size("tp")
    local_tokens, width = tokens.shape
    top_count = route_expert.shape[1]
    capacity = max(2, (local_tokens * top_count * 4 + 3 * experts - 1) // (3 * experts))
    slots = capacity // cores
    pieces = 8 // slots
    piece = width // pieces
    rows = experts * slots * pieces
    sizes = dict(slots=slots, pieces=pieces, experts=experts)

    order = [[seated(block, experts) for block in range(experts)]]
    exchange = functools.partial(
        lax.all_to_all, axis_name="ep", split_axis=0, concat_axis=0, axis_index_groups=order, tiled=True
    )
    swap = [(i, (i + 1) % cores) for i in range(cores)]
    weights = (gate_weight[0], up_weight[0], down_weight[0])
    others = tuple(lax.ppermute(w, "tp", swap) for w in weights[:2])
    others += (lax.ppermute(weights[2], "tp", swap),)

    send, normed = pl.pallas_call(
        functools.partial(dispatch_kernel, **sizes),
        out_shape=(
            pltpu.HBM((rows, piece), BF16),
            VMEM((local_tokens, width), BF16),
        ),
        in_specs=[anywhere()] * 3,
        out_specs=(anywhere(), whole()),
        scratch_shapes=[
            VMEM(tokens.shape, BF16),
            VMEM(in_gain.shape, BF16),
            VMEM(route_expert.shape[::-1], jnp.int32),
            VMEM((rows, piece), BF16),
            pltpu.SemaphoreType.DMA((3,)),
            pltpu.SemaphoreType.DMA((4,)),
        ],
        compiler_params=grant(6),
        name="dispatch",
    )(*far(tokens, in_gain, route_expert.T))
    arrived = exchange(send.reshape(experts, slots * pieces, piece))

    loaded = (shared_gate, shared_up, shared_down, route_expert.T, route_weight.T)
    part, mix = pl.pallas_call(
        functools.partial(side_kernel, **sizes),
        out_shape=(
            VMEM((pieces * local_tokens, piece), F32),
            VMEM((2 * pieces * local_tokens, rows), BF16),
        ),
        in_specs=[whole()] + [anywhere()] * len(loaded),
        out_specs=(whole(), whole()),
        scratch_shapes=[VMEM(w.shape, w.dtype) for w in loaded] + [pltpu.SemaphoreType.DMA((len(loaded),))],
        compiler_params=grant(12),
        name="side",
    )(*held(normed), *far(*loaded))

    inputs, hidden, down = pl.pallas_call(
        functools.partial(opening_kernel, pieces=pieces),
        out_shape=(
            VMEM((rows // pieces, width), BF16),
            VMEM((rows // pieces, weights[0].shape[1]), BF16),
            VMEM(weights[2].shape, BF16),
        ),
        in_specs=[whole()] + [anywhere()] * 3,
        out_specs=(whole(),) * 3,
        scratch_shapes=[VMEM(w.shape, BF16) for w in weights[:2]] + [pltpu.SemaphoreType.DMA((3,))],
        compiler_params=grant(8),
        name="opening",
    )(*held(arrived.reshape(rows, piece)), *far(*weights))

    hidden2, first = pl.pallas_call(
        middle_kernel,
        out_shape=(VMEM(hidden.shape, BF16), VMEM(inputs.shape, F32)),
        in_specs=[whole()] * 3 + [anywhere()] * 2,
        out_specs=(whole(), whole()),
        scratch_shapes=[VMEM(w.shape, BF16) for w in others[:2]] + [pltpu.SemaphoreType.DMA((2,))],
        compiler_params=grant(8),
        name="middle",
    )(*held(inputs, hidden, down), *far(*others[:2]))

    results = pl.pallas_call(
        functools.partial(expert_kernel, pieces=pieces),
        out_shape=VMEM((rows, piece), BF16),
        in_specs=[whole()] * 3,
        out_specs=whole(),
        compiler_params=grant(8),
        name="expert",
    )(*held(hidden2, first, others[2]))
    returned = exchange(results.reshape(experts, slots * pieces, piece))

    mine = pl.pallas_call(
        combine_kernel,
        out_shape=VMEM((pieces * local_tokens, piece), F32),
        in_specs=[whole()] * 3,
        out_specs=whole(),
        compiler_params=grant(4),
        name="combine",
    )(*held(mix, returned.reshape(rows, piece), part))
    other = lax.ppermute(mine, "tp", swap)
    return pl.pallas_call(
        functools.partial(closing_kernel, pieces=pieces),
        out_shape=jax.ShapeDtypeStruct((local_tokens, out_gain.shape[0]), BF16),
        in_specs=[whole()] * 3,
        out_specs=whole(),
        scratch_shapes=[VMEM((pieces * local_tokens, piece), F32)],
        compiler_params=grant(4),
        name="closing",
    )(*held(mine, other, out_gain))


def solution(mesh):
    return jax.shard_map(
        body,
        mesh=mesh,
        in_specs=(
            P(("grp", "ep"), None),
            P(),
            P(("grp", "ep"), None),
            P(("grp", "ep"), None),
            P("ep", None, "tp"),
            P("ep", None, "tp"),
            P("ep", "tp", None),
            P(None, "tp"),
            P(None, "tp"),
            P("tp", None),
            P("tp"),
        ),
        out_specs=P(("grp", "ep"), "tp"),
        check_vma=False,
    )
```

```python
import functools
import math

import jax
import jax.numpy as jnp
from jax import lax
from jax.experimental import pallas as pl
from jax.experimental.pallas import tpu as pltpu
from jax.sharding import PartitionSpec as P


EPSILON = 1e-06
F32 = jnp.float32
BF16 = jnp.bfloat16
VMEM = pltpu.VMEM


def whole():
    return pl.BlockSpec(memory_space=VMEM)


def anywhere():
    return pl.BlockSpec(memory_space=pl.ANY)


def held(*arrays):
    return [pltpu.with_memory_space_constraint(a, VMEM) for a in arrays]


def far(*arrays):
    return [pltpu.with_memory_space_constraint(a, pltpu.HBM) for a in arrays]


def grant(mebibytes):
    return pltpu.CompilerParams(vmem_limit_bytes=mebibytes * 1024 * 1024)


def iota(shape, dim):
    return lax.broadcasted_iota(jnp.int32, shape, dim)


def seated(block, experts):
    side = math.isqrt(experts)
    if side * side != experts or side % 2:
        return block

    def spread(i):
        return i // 2 + i % 2 * (side // 2)

    return experts - 1 - spread(block % side) * side - block // side


def chosen(route, core, slots, pieces, experts, values=None):
    top, tokens = route.shape
    rows, lanes = experts * slots * pieces, pieces * tokens
    row, lane = iota((rows, lanes), 0), iota((rows, lanes), 1)
    expert = seated(row // (slots * pieces), experts)
    tiled = jnp.concatenate([route] * pieces, axis=1)
    hits = [tiled[k : k + 1] == expert for k in range(top)]
    named = functools.reduce(jnp.logical_or, hits)
    before, after = iota((lanes, lanes), 0), iota((lanes, lanes), 1)
    earlier = (before // tokens == after // tokens) & (before < after)
    ones = jnp.where(named, 1.0, 0.0).astype(BF16)
    rank = jnp.dot(ones, jnp.where(earlier, 1.0, 0.0).astype(BF16), preferred_element_type=F32)
    wanted = ((row // pieces) % slots + slots * core).astype(F32)
    keep = named & (rank == wanted) & (lane // tokens == row % pieces)
    if values is None:
        return jnp.where(keep, 1.0, 0.0)
    spread = jnp.concatenate([values] * pieces, axis=1)
    total = jnp.zeros((rows, lanes), F32)
    for k in range(top):
        total = jnp.where(hits[k], spread[k : k + 1], total)
    return jnp.where(keep, total, 0.0)


def dispatch_kernel(
    tokens_hbm,
    gain_hbm,
    route_hbm,
    send_hbm,
    normed_ref,
    tokens_ref,
    gain_ref,
    route_ref,
    send_ref,
    sems,
    out_sems,
    *,
    slots,
    pieces,
    experts,
):
    core = lax.axis_index("tp")
    loads = [
        pltpu.make_async_copy(src, dst, sems.at[i])
        for i, (src, dst) in enumerate(
            ((route_hbm, route_ref), (tokens_hbm, tokens_ref), (gain_hbm, gain_ref))
        )
    ]
    for load in loads:
        load.start()
    for load in loads:
        load.wait()
    pick = chosen(route_ref[...], core, slots, pieces, experts).astype(BF16)
    values = tokens_ref[...].astype(F32)
    scaled = values * lax.rsqrt(jnp.mean(values * values, axis=-1, keepdims=True) + EPSILON)
    normed = (scaled * gain_ref[...].astype(F32)[None, :]).astype(BF16)
    normed_ref[...] = normed
    piece = normed.shape[1] // pieces
    stacked = jnp.concatenate([normed[:, q * piece : (q + 1) * piece] for q in range(pieces)], axis=0)
    chunk = send_ref.shape[0] // 4
    stores = []
    for c in range(4):
        span = slice(c * chunk, (c + 1) * chunk)
        send_ref[span, :] = jnp.dot(pick[span], stacked, preferred_element_type=F32).astype(BF16)
        stores.append(
            pltpu.make_async_copy(
                send_ref.at[pl.ds(c * chunk, chunk)], send_hbm.at[pl.ds(c * chunk, chunk)], out_sems.at[c]
            )
        )
        stores[-1].start()
    for store in stores:
        store.wait()


def gathering(half, pieces):
    to, frm = iota((half * pieces, half * pieces), 0), iota((half * pieces, half * pieces), 1)
    return jnp.where(frm == (to % half) * pieces + to // half, 1.0, 0.0).astype(BF16)


def side_kernel(
    normed_ref,
    shared_gate_hbm,
    shared_up_hbm,
    shared_down_hbm,
    route_hbm,
    weight_hbm,
    kept_hbm,
    part_ref,
    mix_ref,
    kept_ref,
    shared_gate_ref,
    shared_up_ref,
    shared_down_ref,
    route_ref,
    weight_ref,
    sems,
    *,
    slots,
    pieces,
    experts,
):
    core = lax.axis_index("tp")
    pairs = (
        (route_hbm, route_ref),
        (weight_hbm, weight_ref),
        (shared_gate_hbm, shared_gate_ref),
        (shared_up_hbm, shared_up_ref),
        (shared_down_hbm, shared_down_ref),
        (kept_hbm.at[pl.ds(0, kept_ref.shape[0])], kept_ref),
    )
    loads = [pltpu.make_async_copy(src, dst, sems.at[i]) for i, (src, dst) in enumerate(pairs)]
    for load in loads:
        load.start()
    for load in loads[:2]:
        load.wait()
    mix = chosen(route_ref[...], core, slots, pieces, experts, weight_ref[...]).T
    high = mix.astype(BF16)
    mix_ref[: mix.shape[0], :] = high
    mix_ref[mix.shape[0] :, :] = (mix - high.astype(F32)).astype(BF16)
    normed = normed_ref[...]
    tokens, piece = normed.shape[0], normed.shape[1] // pieces
    loads[2].wait()
    gate = jnp.dot(normed, shared_gate_ref[...], preferred_element_type=F32)
    loads[3].wait()
    upward = jnp.dot(normed, shared_up_ref[...], preferred_element_type=F32)
    hidden = (gate * jax.nn.sigmoid(gate) * upward).astype(BF16)
    loads[4].wait()
    for q in range(pieces):
        part_ref[q * tokens : (q + 1) * tokens, :] = jnp.dot(
            hidden, shared_down_ref[:, q * piece : (q + 1) * piece], preferred_element_type=F32
        )
    loads[5].wait()


def opening_kernel(
    rows_ref,
    kept_ref,
    gate_hbm,
    up_hbm,
    down_hbm,
    inputs_ref,
    hidden_ref,
    down_ref,
    gate_ref,
    up_ref,
    sems,
    *,
    pieces,
):
    kept, rest = kept_ref.shape[0], gate_ref.shape[0]
    pairs = ((gate_hbm.at[pl.ds(kept, rest)], gate_ref), (up_hbm, up_ref), (down_hbm, down_ref))
    loads = [pltpu.make_async_copy(src, dst, sems.at[i]) for i, (src, dst) in enumerate(pairs)]
    for load in loads:
        load.start()
    total = rows_ref.shape[0]
    block, half = total // 2, total // pieces // 2
    piece = rows_ref.shape[1]
    order = gathering(half, pieces)
    for h in range(2):
        part = jnp.dot(order, rows_ref[h * block : (h + 1) * block, :], preferred_element_type=F32).astype(BF16)
        for q in range(pieces):
            inputs_ref[h * half : (h + 1) * half, q * piece : (q + 1) * piece] = part[q * half : (q + 1) * half]
    inputs = inputs_ref[...]
    gate = jnp.dot(inputs[:, :kept], kept_ref[...], preferred_element_type=F32)
    loads[0].wait()
    gate += jnp.dot(inputs[:, kept:], gate_ref[...], preferred_element_type=F32)
    loads[1].wait()
    upward = jnp.dot(inputs, up_ref[...], preferred_element_type=F32)
    hidden_ref[...] = (gate * jax.nn.sigmoid(gate) * upward).astype(BF16)
    loads[2].wait()


def middle_kernel(
    inputs_ref, hidden_ref, down_ref, gate2_hbm, up2_hbm, hidden2_ref, first_ref, gate2_ref, up2_ref, sems
):
    pairs = ((gate2_hbm, gate2_ref), (up2_hbm, up2_ref))
    loads = [pltpu.make_async_copy(src, dst, sems.at[i]) for i, (src, dst) in enumerate(pairs)]
    for load in loads:
        load.start()
    first_ref[...] = jnp.dot(hidden_ref[...], down_ref[...], preferred_element_type=F32)
    inputs = inputs_ref[...]
    loads[0].wait()
    gate = jnp.dot(inputs, gate2_ref[...], preferred_element_type=F32)
    loads[1].wait()
    upward = jnp.dot(inputs, up2_ref[...], preferred_element_type=F32)
    hidden2_ref[...] = (gate * jax.nn.sigmoid(gate) * upward).astype(BF16)


def expert_kernel(hidden2_ref, first_ref, down2_ref, out_ref, *, pieces):
    total, piece = out_ref.shape
    block, half = total // 2, total // pieces // 2
    back = gathering(half, pieces).T
    hidden2 = hidden2_ref[...]
    results = []
    for q in range(pieces):
        span = slice(q * piece, (q + 1) * piece)
        results.append(
            (
                first_ref[:, span] + jnp.dot(hidden2, down2_ref[:, span], preferred_element_type=F32)
            ).astype(BF16)
        )
    for h in range(2):
        lined = jnp.concatenate([r[h * half : (h + 1) * half] for r in results], axis=0)
        out_ref[h * block : (h + 1) * block, :] = jnp.dot(back, lined, preferred_element_type=F32).astype(BF16)


def combine_kernel(mix_ref, returned_ref, part_ref, out_ref):
    both = jnp.dot(mix_ref[...], returned_ref[...], preferred_element_type=F32)
    size = both.shape[0] // 2
    out_ref[...] = part_ref[...] + both[:size] + both[size:]


def closing_kernel(mine_ref, other_ref, gain_ref, out_ref, total_ref, *, pieces):
    core = lax.axis_index("tp")
    total = mine_ref[...] + other_ref[...]
    total_ref[...] = total
    tokens, piece = total.shape[0] // pieces, total.shape[1]
    squares = jnp.sum(total * total, axis=1, keepdims=True)
    squares = functools.reduce(jnp.add, [squares[q * tokens : (q + 1) * tokens] for q in range(pieces)])
    scale = lax.rsqrt(squares / (pieces * piece) + EPSILON)
    mine = out_ref.shape[1] // piece
    gain = gain_ref[...].astype(F32)[None, :]
    for q in range(mine):
        start = pl.multiple_of((core * mine + q) * tokens, 8)
        values = total_ref[pl.ds(start, tokens), :] * scale
        out_ref[:, q * piece : (q + 1) * piece] = (values * gain[:, q * piece : (q + 1) * piece]).astype(BF16)


def body(
    tokens,
    in_gain,
    route_expert,
    route_weight,
    gate_weight,
    up_weight,
    down_weight,
    shared_gate,
    shared_up,
    shared_down,
    out_gain,
):
    experts, cores = lax.axis_size("ep"), lax.axis_size("tp")
    local_tokens, width = tokens.shape
    top_count = route_expert.shape[1]
    capacity = max(2, (local_tokens * top_count * 4 + 3 * experts - 1) // (3 * experts))
    slots = capacity // cores
    pieces = 8 // slots
    piece = width // pieces
    rows = experts * slots * pieces
    sizes = dict(slots=slots, pieces=pieces, experts=experts)

    order = [[seated(block, experts) for block in range(experts)]]
    exchange = functools.partial(
        lax.all_to_all, axis_name="ep", split_axis=0, concat_axis=0, axis_index_groups=order, tiled=True
    )
    swap = [(i, (i + 1) % cores) for i in range(cores)]
    weights = (gate_weight[0], up_weight[0], down_weight[0])
    others = tuple(lax.ppermute(w, "tp", swap) for w in weights[:2])
    others += (lax.ppermute(weights[2], "tp", swap),)

    send, normed = pl.pallas_call(
        functools.partial(dispatch_kernel, **sizes),
        out_shape=(
            pltpu.HBM((rows, piece), BF16),
            VMEM((local_tokens, width), BF16),
        ),
        in_specs=[anywhere()] * 3,
        out_specs=(anywhere(), whole()),
        scratch_shapes=[
            VMEM(tokens.shape, BF16),
            VMEM(in_gain.shape, BF16),
            VMEM(route_expert.shape[::-1], jnp.int32),
            VMEM((rows, piece), BF16),
            pltpu.SemaphoreType.DMA((3,)),
            pltpu.SemaphoreType.DMA((4,)),
        ],
        compiler_params=grant(6),
        name="dispatch",
    )(*far(tokens, in_gain, route_expert.T))
    arrived = exchange(send.reshape(experts, slots * pieces, piece))

    loaded = (shared_gate, shared_up, shared_down, route_expert.T, route_weight.T)
    part, mix, kept = pl.pallas_call(
        functools.partial(side_kernel, **sizes),
        out_shape=(
            VMEM((pieces * local_tokens, piece), F32),
            VMEM((2 * pieces * local_tokens, rows), BF16),
            VMEM((weights[0].shape[0] // 2, weights[0].shape[1]), BF16),
        ),
        in_specs=[whole()] + [anywhere()] * 6,
        out_specs=(whole(),) * 3,
        scratch_shapes=[VMEM(w.shape, w.dtype) for w in loaded] + [pltpu.SemaphoreType.DMA((6,))],
        compiler_params=grant(12),
        name="side",
    )(*held(normed), *far(*loaded, weights[0]))

    inputs, hidden, down = pl.pallas_call(
        functools.partial(opening_kernel, pieces=pieces),
        out_shape=(
            VMEM((rows // pieces, width), BF16),
            VMEM((rows // pieces, weights[0].shape[1]), BF16),
            VMEM(weights[2].shape, BF16),
        ),
        in_specs=[whole()] * 2 + [anywhere()] * 3,
        out_specs=(whole(),) * 3,
        scratch_shapes=[VMEM(kept.shape, BF16), VMEM(weights[1].shape, BF16), pltpu.SemaphoreType.DMA((3,))],
        compiler_params=grant(8),
        name="opening",
    )(*held(arrived.reshape(rows, piece), kept), *far(*weights))

    hidden2, first = pl.pallas_call(
        middle_kernel,
        out_shape=(VMEM(hidden.shape, BF16), VMEM(inputs.shape, F32)),
        in_specs=[whole()] * 3 + [anywhere()] * 2,
        out_specs=(whole(), whole()),
        scratch_shapes=[VMEM(w.shape, BF16) for w in others[:2]] + [pltpu.SemaphoreType.DMA((2,))],
        compiler_params=grant(8),
        name="middle",
    )(*held(inputs, hidden, down), *far(*others[:2]))

    results = pl.pallas_call(
        functools.partial(expert_kernel, pieces=pieces),
        out_shape=VMEM((rows, piece), BF16),
        in_specs=[whole()] * 3,
        out_specs=whole(),
        compiler_params=grant(8),
        name="expert",
    )(*held(hidden2, first, others[2]))
    returned = exchange(results.reshape(experts, slots * pieces, piece))

    mine = pl.pallas_call(
        combine_kernel,
        out_shape=VMEM((pieces * local_tokens, piece), F32),
        in_specs=[whole()] * 3,
        out_specs=whole(),
        compiler_params=grant(4),
        name="combine",
    )(*held(mix, returned.reshape(rows, piece), part))
    other = lax.ppermute(mine, "tp", swap)
    return pl.pallas_call(
        functools.partial(closing_kernel, pieces=pieces),
        out_shape=jax.ShapeDtypeStruct((local_tokens, out_gain.shape[0]), BF16),
        in_specs=[whole()] * 3,
        out_specs=whole(),
        scratch_shapes=[VMEM((pieces * local_tokens, piece), F32)],
        compiler_params=grant(4),
        name="closing",
    )(*held(mine, other, out_gain))


def solution(mesh):
    return jax.shard_map(
        body,
        mesh=mesh,
        in_specs=(
            P(("grp", "ep"), None),
            P(),
            P(("grp", "ep"), None),
            P(("grp", "ep"), None),
            P("ep", None, "tp"),
            P("ep", None, "tp"),
            P("ep", "tp", None),
            P(None, "tp"),
            P(None, "tp"),
            P("tp", None),
            P("tp"),
        ),
        out_specs=P(("grp", "ep"), "tp"),
        check_vma=False,
    )
```
